32 devices in a mesh: rep: 2 (over x), fs: 8 (over z, y), tp: 2 (over core).
Axes of the slice: x: 2, y: 2, z: 4, core: 2. Of those that a mesh axis runs over, the one named last changes fastest.
Arguments:
- tokens: bfloat16 [5120, 2048], P(('rep', 'fs')), may hold values from -6 to 6
- gate_weight: float32 [2048, 5120], P('fs', 'tp'), may hold values from -0.125 to 0.125
- up_weight: float32 [2048, 5120], P('fs', 'tp'), may hold values from -0.125 to 0.125
- down_weight: float32 [2048, 5120], P('fs', 'tp'), may hold values from -0.078125 to 0.078125
- value_weight: float32 [2048, 2048], P('fs', 'tp'), may hold values from -0.125 to 0.125
- glu_weight: float32 [2048, 2048], P('fs', 'tp'), may hold values from -0.125 to 0.125
- out_weight: float32 [2048, 2048], P('fs', 'tp'), may hold values from -0.125 to 0.125
- gate_scale: float32 [5120], P('tp'), may hold values from 0.1 to 1.9
- up_scale: float32 [5120], P('tp'), may hold values from 0.5 to 2
- down_scale: float32 [2048], P('fs'), may hold values from 1 to 4
- value_scale: float32 [2048], P('tp'), may hold values from 0.2 to 3.4
- glu_scale: float32 [2048], P('tp'), may hold values from 0.1 to 1.9
- out_scale: float32 [2048], P('fs'), may hold values from 1 to 4
- conv_kernel: float32 [31, 2048], P(None, 'tp'), may hold values from -1 to 1
- norm_gain: float32 [2048], P('tp'), may hold values from 0.1 to 1.9
- first_gain: float32 [2048], replicated, may hold values from 0.1 to 1.9
- conv_gain: float32 [2048], replicated, may hold values from 0.1 to 1.9
- second_gain: float32 [2048], replicated, may hold values from 0.1 to 1.9
Outputs:
- result: bfloat16 [5120, 2048], P(('rep', 'fs'))
The draws below stay inside these ranges and needn't reach their ends.
All inputs are finite; a program needn't handle non-finite values.
Results may differ from the reference program's by a relative error of at most 0.02.
Values may be sent and summed in bfloat16 or wider, within the bound.
A program may use at most 128 MiB of HBM per device.

```python
import math
import jax
import jax.numpy as jnp
from jax import lax

D = 2048
FF = 5120
KW = 31
SEQ = 320
TOKENS = 5120
N_REP = 2
N_FS = 8
N_TP = 2


def draw_value_scale(key, part):
    position = jnp.arange(D, dtype=jnp.float32) / D
    noise = jax.random.uniform(key, (D,), jnp.float32, 0.7, 1.4)
    ramp = 0.5 * jnp.exp(jnp.log(4.0) * position)
    return (ramp * noise).astype(jnp.float32)


def shard_levels(rng, shape, pieces, least, high):
    level, own = 1.0, jax.random.fold_in(rng, 6)
    for dim, blocks in pieces:
        draws = jnp.exp(jax.random.uniform(jax.random.fold_in(own, dim), (blocks,), jnp.float32, least / len(pieces), high / len(pieces)))
        level = level * jnp.repeat(draws, shape[dim] // blocks).reshape([-1 if axis == dim else 1 for axis in range(len(shape))])
    return level


def scatter_about(own_key, extent, scale, most, shards=(), kind=jnp.bfloat16):
    array = jax.random.normal(own_key, extent, jnp.float32) * scale
    if len(shards) > 0:
        array = shard_levels(own_key, extent, shards, -0.22, 0.18) * array
    return jnp.clip(array, min=-most, max=most).astype(kind)


def setup_inputs(seed: int = 0) -> dict:
    key_of = jax.random.split(jax.random.key(seed), 19)
    return {
        "tokens": scatter_about(key_of[0], (TOKENS, D), 1.0, 6.0, ((0, 16),)),
        "gate_weight": scatter_about(key_of[1], (D, FF), D ** -0.5, 0.125, ((0, 8), (1, 2)), jnp.float32),
        "up_weight": scatter_about(key_of[2], (D, FF), D ** -0.5, 0.125, ((0, 8), (1, 2)), jnp.float32),
        "down_weight": scatter_about(key_of[3], (D, FF), FF ** -0.5, 0.078125, ((0, 8), (1, 2)), jnp.float32),
        "value_weight": scatter_about(key_of[4], (D, D), D ** -0.5, 0.125, ((0, 8), (1, 2)), jnp.float32),
        "glu_weight": scatter_about(key_of[5], (D, D), D ** -0.5, 0.125, ((0, 8), (1, 2)), jnp.float32),
        "out_weight": scatter_about(key_of[6], (D, D), D ** -0.5, 0.125, ((0, 8), (1, 2)), jnp.float32),
        "gate_scale": jnp.clip(1.0 + 0.18 * jax.random.normal(key_of[7], (FF,), jnp.float32), 0.1, 1.9),
        "up_scale": jnp.clip(jnp.exp(math.log(2.0) - 1.3862944 * jax.random.uniform(key_of[8], (FF,), jnp.float32) ** shard_levels(key_of[8], (FF,), ((0, 2),), -0.2, 0.2)), 0.5, 2.0),
        "down_scale": jnp.clip(jnp.exp(math.log(4.0) - 1.3862944 * jax.random.uniform(key_of[9], (D,), jnp.float32) ** shard_levels(key_of[9], (D,), ((0, 8),), -0.2, 0.2)), 1.0, 4.0),
        "value_scale": draw_value_scale(jax.random.fold_in(key_of[18], 71), 0),
        "glu_scale": jnp.clip(1.0 + 0.18 * jax.random.normal(key_of[11], (D,), jnp.float32), 0.1, 1.9),
        "out_scale": jnp.clip(jnp.exp(math.log(4.0) - 1.3862944 * jax.random.uniform(key_of[12], (D,), jnp.float32) ** shard_levels(key_of[12], (D,), ((0, 8),), -0.2, 0.2)), 1.0, 4.0),
        "conv_kernel": scatter_about(key_of[13], (KW, D), KW ** -0.5, 1.0, ((1, 2),), jnp.float32),
        "norm_gain": jnp.clip(1.0 + 0.18 * jax.random.normal(key_of[14], (D,), jnp.float32), 0.1, 1.9),
        "first_gain": jnp.clip(1.0 + 0.18 * jax.random.normal(key_of[15], (D,), jnp.float32), 0.1, 1.9),
        "conv_gain": jnp.clip(1.0 + 0.18 * jax.random.normal(key_of[16], (D,), jnp.float32), 0.1, 1.9),
        "second_gain": jnp.clip(1.0 + 0.18 * jax.random.normal(key_of[17], (D,), jnp.float32), 0.1, 1.9),
    }


EPSILON = 1e-06

def rms_rows(rows, gains):
    values = rows.astype(jnp.float32)
    scaled = values * lax.rsqrt(lax.optimization_barrier(jnp.mean(values * values, axis=-1, keepdims=True)) + EPSILON)
    return (scaled * gains).astype(jnp.bfloat16)

def gated_hidden(normed, gate_full, up_full, gate_scale, up_scale):
    gate_part = jnp.dot(normed, gate_full, preferred_element_type=jnp.float32) * gate_scale
    upward = jnp.dot(normed, up_full, preferred_element_type=jnp.float32) * up_scale
    return (jax.nn.silu(gate_part) * upward).astype(jnp.bfloat16)

def block_sum(active, weight_rows):
    width = active.shape[1] // N_TP
    total = jnp.zeros((active.shape[0], weight_rows.shape[0]), jnp.float32)
    for block in range(N_TP):
        partial_term = lax.dot_general(active[:, block * width:(block + 1) * width], weight_rows[:, block * width:(block + 1) * width], (((1,), (1,)), ((), ())), preferred_element_type=jnp.float32)
        rounded = lax.optimization_barrier(partial_term.astype(jnp.bfloat16))
        total = total + rounded.astype(jnp.float32)
    return total

def causal_depthwise(inputs, kernel):
    taps = kernel.shape[0]
    length = inputs.shape[0]
    padded = jnp.concatenate([jnp.zeros((taps - 1, inputs.shape[1]), jnp.float32), inputs.astype(jnp.float32)], axis=0)
    total = jnp.zeros((length, inputs.shape[1]), jnp.float32)
    for offset in range(taps):
        total = total + kernel[offset] * padded[offset:offset + length]
    return total

def reference(tokens, gate_weight, up_weight, down_weight, value_weight, glu_weight, out_weight, gate_scale, up_scale, down_scale, value_scale, glu_scale, out_scale, conv_kernel, norm_gain, first_gain, conv_gain, second_gain):
    gate_full = gate_weight.astype(jnp.bfloat16)
    up_full = up_weight.astype(jnp.bfloat16)
    down_full = down_weight.astype(jnp.bfloat16)
    value_full = value_weight.astype(jnp.bfloat16)
    glu_full = glu_weight.astype(jnp.bfloat16)
    out_full = out_weight.astype(jnp.bfloat16)

    def one_sequence(rows):
        hidden = gated_hidden(rms_rows(rows, first_gain), gate_full, up_full, gate_scale, up_scale)
        after_first = (rows.astype(jnp.float32) + 0.5 * down_scale * block_sum(hidden, down_full)).astype(jnp.bfloat16)
        normed = rms_rows(after_first, conv_gain)
        value_part = jnp.dot(normed, value_full, preferred_element_type=jnp.float32) * value_scale
        gate_part = jnp.dot(normed, glu_full, preferred_element_type=jnp.float32) * glu_scale
        glu_in = (value_part * jax.nn.sigmoid(gate_part)).astype(jnp.bfloat16)
        mixed = causal_depthwise(glu_in, conv_kernel)
        mean_rows = lax.optimization_barrier(jnp.mean(mixed, axis=1, keepdims=True))
        square_rows = lax.optimization_barrier(jnp.mean(mixed * mixed, axis=1, keepdims=True))
        normalized = (mixed - mean_rows) * lax.rsqrt(square_rows - mean_rows * mean_rows + EPSILON) * norm_gain
        active = jax.nn.silu(normalized).astype(jnp.bfloat16)
        after_conv = (after_first.astype(jnp.float32) + out_scale * block_sum(active, out_full)).astype(jnp.bfloat16)
        hidden = gated_hidden(rms_rows(after_conv, second_gain), gate_full, up_full, gate_scale, up_scale)
        return (after_conv.astype(jnp.float32) + 0.5 * down_scale * block_sum(hidden, down_full)).astype(jnp.bfloat16)
    groups = tokens.reshape(N_REP * N_FS, SEQ, D)
    return lax.map(one_sequence, groups).reshape(TOKENS, D)
```

```python
import functools

import jax
import jax.numpy as jnp
from jax import lax
from jax.experimental import pallas as pl
from jax.experimental.pallas import tpu as pltpu
from jax.sharding import PartitionSpec as P

MESH = pl.DeviceIdType.MESH
EPSILON = 1e-06
LANES = 128
TILE = 256
ROWS = 16
NT = (((1,), (1,)), ((), ()))
TN = (((0,), (0,)), ((), ()))


def fused_kernel(dims, *refs):
    S, D, H, C, KW, F, RX = dims
    Z = F // 2
    SH = S // 2
    R = 2 * RX
    PAD = -(-(KW - 1) // 8) * 8
    (tokens, m0, m1, m2, m3, t0, t1, t2, t3, sc_in, first_gain, conv_gain, second_gain, gate_scale, up_scale,
     value_scale, glu_scale, norm_gain, conv_k, out, *scratch) = refs
    (wb0, wb1, wb2, wb3, tokv, xa, xb, xc, hid, part, rc, ry, ys, res, gp, mixed, act, st, scl, dsc,
     loc_sem, y_send, y_recv, u_send, d_send, z_recv, x_send, x_recv, tok_sem, s_send, s_recv,
     rc_send, rc_recv, ry_send, ry_recv, ag_send, ag_recv, st_send, st_recv, out_sem) = scratch
    mine, theirs, wb = (m0, m1, m2, m3), (t0, t1, t2, t3), (wb0, wb1, wb2, wb3)
    G = len(wb)

    x = lax.axis_index("rep")
    f = lax.axis_index("fs")
    c = lax.axis_index("tp")
    y = lax.rem(f, 2)
    z = lax.div(f, 2)
    fp = f + 1 - 2 * y
    ox, oy, oc = 1 - x, 1 - y, 1 - c
    dx, dc, dy, dyc = {"rep": ox}, {"tp": oc}, {"fs": fp}, {"fs": fp, "tp": oc}
    up, dn = {"fs": f + 2}, {"fs": f - 2}

    def rcopy(src, dst, ssem, rsem, dev):
        return pltpu.make_async_remote_copy(
            src_ref=src, dst_ref=dst, send_sem=ssem, recv_sem=rsem, device_id=dev, device_id_type=MESH
        )

    barrier = pltpu.get_barrier_semaphore()
    for j in range(1, F):
        pl.semaphore_signal(barrier, inc=1, device_id={"fs": lax.rem(f + j, F)}, device_id_type=MESH)
    for dev in (dx, dc, dyc):
        pl.semaphore_signal(barrier, inc=1, device_id=dev, device_id_type=MESH)
    pl.semaphore_wait(barrier, F + 2)

    def y_copy(g, h):
        return rcopy(theirs[g].at[h], wb[g].at[2 * f + h], y_send.at[g, h], y_recv.at[g, h], dy)

    def y_wait(g, h):
        b = wb[g].at[2 * fp + h]
        rcopy(b, b, y_send.at[g, h], y_recv.at[g, h], dy).wait_recv()

    def z_copy(g, q, sems, dev, own=False):
        b = wb[g].at[2 * q + x]
        return rcopy(mine[g].at[x] if own else b, b, sems.at[g, q], z_recv.at[g, q], dev)

    def x_copy(g, q):
        b = wb[g].at[2 * q + x]
        return rcopy(b, b, x_send.at[g, q], x_recv.at[g, q], dx)

    def local_copy(g):
        return pltpu.make_async_copy(mine[g], wb[g].at[pl.ds(2 * f, 2)], loc_sem.at[g])

    def send_own(g):
        @pl.when(z < Z - 1)
        def _():
            z_copy(g, f, u_send, up, True).start()

        @pl.when(z > 0)
        def _():
            z_copy(g, f, d_send, dn, True).start()

    def send_pair(g):
        y_wait(g, x)

        @pl.when(z < Z - 1)
        def _():
            z_copy(g, fp, u_send, up).start()

        @pl.when(z > 0)
        def _():
            z_copy(g, fp, d_send, dn).start()

    def forward(g, d):
        for k in range(2):
            yy = y if k == 0 else oy

            @pl.when(z >= d)
            def _():
                q = 2 * (z - d) + yy
                z_copy(g, q, u_send, up).wait_recv()

                @pl.when(z < Z - 1)
                def _():
                    z_copy(g, q, u_send, up).start()

                x_copy(g, q).start()

            @pl.when(z + d < Z)
            def _():
                q = 2 * (z + d) + yy
                z_copy(g, q, d_send, dn).wait_recv()

                @pl.when(z > 0)
                def _():
                    z_copy(g, q, d_send, dn).start()

                x_copy(g, q).start()

    def group_done(g):
        local_copy(g).wait()
        y_wait(g, ox)
        for d in range(1, Z):
            for yy in range(2):
                for side in (-1, 1):
                    @pl.when((z >= d) if side < 0 else (z + d < Z))
                    def _():
                        q = 2 * (z + side * d) + yy
                        b = wb[g].at[2 * q + ox]
                        rcopy(b, b, x_send.at[g, q], x_recv.at[g, q], dx).wait_recv()

    def drain(g):
        for h in range(2):
            y_copy(g, h).wait_send()
        for q in range(F):
            zq = q // 2

            @pl.when((z < Z - 1) & (zq <= z))
            def _():
                z_copy(g, q, u_send, up).wait_send()

            @pl.when((z > 0) & (zq >= z))
            def _():
                z_copy(g, q, d_send, dn).wait_send()

            @pl.when(zq != z)
            def _():
                x_copy(g, q).wait_send()

    y_copy(0, x).start()
    send_own(0)
    tok_local = pltpu.make_async_copy(tokens, tokv.at[y], out_sem.at[2])
    tok_local.start()
    for g in range(1, G):
        y_copy(g, x).start()
    for g in range(G):
        local_copy(g).start()
    y_copy(0, ox).start()
    tok_y = rcopy(tokens, tokv.at[y], tok_sem.at[0], tok_sem.at[1], dy)
    tok_y.start()
    for g in range(1, G):
        y_copy(g, ox).start()
    own_scale = pltpu.make_async_copy(sc_in, scl.at[f], out_sem.at[3])
    own_scale.start()
    for j in range(1, F):
        rcopy(sc_in, scl.at[f], s_send.at[j], s_recv.at[f], {"fs": lax.rem(f + j, F)}).start()

    def norm(v, gains):
        return (v * lax.rsqrt(jnp.mean(v * v, axis=-1, keepdims=True) + EPSILON) * gains).astype(jnp.bfloat16)

    def norm_tokens(s):
        @pl.loop(0, S // ROWS)
        def _(i):
            r = pl.ds(i * ROWS, ROWS)
            xa[s, r, :] = norm(tokv[s, r, :].astype(jnp.float32), first_gain[...])

    def gate_up(src, s):
        @pl.loop(0, H // TILE)
        def _(j):
            lo = pl.multiple_of(j * TILE, TILE)
            a = src[s]
            gw = wb0[:, :, pl.ds(lo, TILE)].reshape(D, TILE)
            uw = wb0[:, :, pl.ds(H + lo, TILE)].reshape(D, TILE)
            gv = jnp.dot(a, gw, preferred_element_type=jnp.float32) * gate_scale[:, pl.ds(lo, TILE)]
            uv = jnp.dot(a, uw, preferred_element_type=jnp.float32) * up_scale[:, pl.ds(lo, TILE)]
            hid[s, :, pl.ds(lo, TILE)] = (gv * jax.nn.sigmoid(gv) * uv).astype(jnp.bfloat16)

    def project(src, w, width, s):
        @pl.loop(0, F)
        def _(j):
            rows = w[pl.ds(2 * j, 2)].reshape(R, width)
            p = lax.dot_general(src[s], rows, NT, preferred_element_type=jnp.float32)
            part[s, :, pl.ds(pl.multiple_of(j * R, R), R)] = p.astype(jnp.bfloat16)

    crows = pl.ds(c * SH, SH)
    orows = pl.ds(oc * SH, SH)

    def rs_core(u, s):
        return rcopy(part.at[s, orows], rc.at[u, s], rc_send.at[u, s], rc_recv.at[u, s], dc)

    def rs_pair(u):
        return rcopy(ys.at[u], ry.at[u], ry_send.at[u], ry_recv.at[u], dy)

    def rs_push(u):
        rs_core(u, oy).wait_recv()

        @pl.loop(0, SH // ROWS)
        def _(i):
            r = pl.ds(i * ROWS, ROWS)
            p = part[oy, pl.ds(c * SH + i * ROWS, ROWS), :].astype(jnp.float32)
            ys[u, r, :] = (p + rc[u, oy, r, :].astype(jnp.float32)).astype(jnp.bfloat16)

        rs_pair(u).start()

    def rs_finish(u, base, factor, scale_row, gains, dst):
        rs_core(u, y).wait_recv()
        rs_pair(u).wait_recv()
        sc = dsc[scale_row:scale_row + 1, :] * factor

        @pl.loop(0, SH // ROWS)
        def _(i):
            r = pl.ds(i * ROWS, ROWS)
            rr = pl.ds(c * SH + i * ROWS, ROWS)
            total = part[y, rr, :].astype(jnp.float32) + rc[u, y, r, :].astype(jnp.float32)
            total = total + ry[u, r, :].astype(jnp.float32)
            b = tokv[y, rr, :] if base is None else res[base, r, :]
            now = (b.astype(jnp.float32) + sc * total).astype(jnp.bfloat16)
            res[u, r, :] = now
            if dst is not None:
                dst[y, rr, :] = norm(now.astype(jnp.float32), gains[...])

    def ag_core(u, buf):
        b = buf.at[y, crows]
        return rcopy(b, b, ag_send.at[u, 0], ag_recv.at[u, 0], dc)

    def ag_pair(u, buf):
        b = buf.at[y, crows]
        return rcopy(b, b, ag_send.at[u, 1], ag_recv.at[u, 1], dy)

    def ag_relay(u, buf):
        b = buf.at[oy, crows]
        return rcopy(b, b, ag_send.at[u, 2], ag_recv.at[u, 2], dc)

    def ag_wait(u, k, buf, s, rows):
        b = buf.at[s, rows]
        rcopy(b, b, ag_send.at[u, k], ag_recv.at[u, k], dc).wait_recv()

    def ag_start(u, buf):
        ag_pair(u, buf).start()
        ag_core(u, buf).start()

    def ag_pass(u, buf):
        ag_wait(u, 1, buf, oy, crows)
        ag_relay(u, buf).start()
        ag_wait(u, 0, buf, y, orows)

    def value_glu(s):
        @pl.loop(0, C // TILE)
        def _(j):
            lo = pl.multiple_of(j * TILE, TILE)
            a = xb[s]
            vw = wb2[:, :, pl.ds(lo, TILE)].reshape(D, TILE)
            gw = wb2[:, :, pl.ds(C + lo, TILE)].reshape(D, TILE)
            vv = jnp.dot(a, vw, preferred_element_type=jnp.float32) * value_scale[:, pl.ds(lo, TILE)]
            gv = jnp.dot(a, gw, preferred_element_type=jnp.float32) * glu_scale[:, pl.ds(lo, TILE)]
            g = (vv * jax.nn.sigmoid(gv)).astype(jnp.bfloat16)
            gp[s, pl.ds(PAD, S), pl.ds(lo, TILE)] = g.astype(jnp.float32)

    def convolve(s):
        @pl.loop(0, C // LANES)
        def _(j):
            cols = pl.ds(pl.multiple_of(j * LANES, LANES), LANES)
            gp[s, pl.ds(0, PAD), cols] = jnp.zeros((PAD, LANES), jnp.float32)
            total = jnp.zeros((S, LANES), jnp.float32)
            for k in range(KW):
                total = total + conv_k[k:k + 1, cols] * gp[s, pl.ds(PAD - (KW - 1) + k, S), cols]
            mixed[s, :, cols] = total

        m = mixed[s]
        low = lax.broadcasted_iota(jnp.int32, (8, C), 0) < 4
        one, nil = jnp.ones((8, C), jnp.float32), jnp.zeros((8, C), jnp.float32)
        hi = lax.Precision.HIGHEST
        sums = lax.dot_general(jnp.where(low, one, nil), m, NT, precision=hi, preferred_element_type=jnp.float32)
        squares = lax.dot_general(jnp.where(low, nil, one), m * m, NT, precision=hi, preferred_element_type=jnp.float32)
        st[0, s] = sums + squares

    def st_copies():
        return [rcopy(st.at[0], st.at[k + 1], st_send.at[k], st_recv.at[k], dev) for k, dev in enumerate((dc, dy, dyc))]

    def activate(s):
        total = st[0, s] + st[1, s] + st[2, s] + st[3, s]
        total = total / D
        mean, square = total[0:1], total[4:5]
        rstd = lax.rsqrt(square - mean * mean + EPSILON)
        row = lax.broadcasted_iota(jnp.int32, (8, S), 0)
        both = jnp.where(row == 0, jnp.broadcast_to(mean, (8, S)), jnp.where(row == 1, jnp.broadcast_to(rstd, (8, S)), 0.0))
        pick = lax.broadcasted_iota(jnp.int32, (8, LANES), 0)
        hi = lax.Precision.HIGHEST
        mcol = lax.dot_general(both, jnp.where(pick == 0, 1.0, 0.0), TN, precision=hi, preferred_element_type=jnp.float32)
        rcol = lax.dot_general(both, jnp.where(pick == 1, 1.0, 0.0), TN, precision=hi, preferred_element_type=jnp.float32)
        for j in range(C // LANES):
            cols = slice(j * LANES, (j + 1) * LANES)
            v = (mixed[s, :, cols] - mcol) * rcol * norm_gain[:, cols]
            act[s, :, cols] = (v * jax.nn.sigmoid(v)).astype(jnp.bfloat16)

    def own_and_pair(g):
        send_own(g)
        send_pair(g)

    send_pair(0)
    tok_local.wait()
    norm_tokens(y)
    forward(0, 1)
    for d in range(2, Z - 1):
        forward(0, d)
    own_and_pair(1)
    tok_y.wait_recv()
    norm_tokens(oy)
    forward(0, Z - 1)
    forward(1, 1)
    group_done(0)
    gate_up(xa, oy)
    for d in range(2, Z - 1):
        forward(1, d)
    own_and_pair(2)
    gate_up(xa, y)
    forward(1, Z - 1)
    forward(2, 1)
    group_done(1)
    project(hid, wb1, H, oy)
    rs_core(0, oy).start()
    project(hid, wb1, H, y)
    rs_core(0, y).start()
    rs_push(0)
    own_scale.wait()
    for j in range(1, F):
        b = scl.at[lax.rem(f + j, F)]
        rcopy(b, b, s_send.at[j], s_recv.at[lax.rem(f + j, F)], dy).wait_recv()
    for j in range(F):
        dsc[:, j * R:(j + 1) * R] = scl[j]
    for d in range(2, Z - 1):
        forward(2, d)
    own_and_pair(3)
    forward(2, Z - 1)
    forward(3, 1)
    rs_finish(0, None, 0.5, 0, conv_gain, xb)
    ag_start(0, xb)
    for d in range(2, Z):
        forward(3, d)
    ag_pass(0, xb)
    group_done(2)
    value_glu(y)
    convolve(y)
    ag_wait(0, 2, xb, oy, orows)
    value_glu(oy)
    convolve(oy)
    for cp in st_copies():
        cp.start()
    for s in range(2):
        rs_core(0, s).wait_send()
    for cp in st_copies():
        cp.wait()
    group_done(3)
    activate(oy)
    project(act, wb3, C, oy)
    rs_core(1, oy).start()
    activate(y)
    project(act, wb3, C, y)
    rs_core(1, y).start()
    rs_push(1)
    rs_finish(1, 0, 1.0, 1, second_gain, xc)
    ag_start(1, xc)
    ag_pass(1, xc)
    gate_up(xc, y)
    for s in range(2):
        rs_core(1, s).wait_send()
    ag_wait(1, 2, xc, oy, orows)
    gate_up(xc, oy)
    project(hid, wb1, H, oy)
    rs_core(2, oy).start()
    project(hid, wb1, H, y)
    rs_core(2, y).start()
    rs_push(2)
    rs_finish(2, 1, 0.5, 0, None, None)
    out_local = pltpu.make_async_copy(res.at[2], out.at[crows], out_sem.at[0])
    out_local.start()
    out_core = rcopy(res.at[2], out.at[crows], tok_sem.at[2], out_sem.at[1], dc)
    out_core.start()
    for g in range(G):
        drain(g)
    tok_y.wait_send()
    for j in range(1, F):
        rcopy(sc_in, scl.at[f], s_send.at[j], s_recv.at[f], dy).wait_send()
    for s in range(2):
        rs_core(2, s).wait_send()
    for u in range(3):
        rs_pair(u).wait_send()
    for u, buf in enumerate((xb, xc)):
        ag_core(u, buf).wait_send()
        ag_pair(u, buf).wait_send()
        ag_relay(u, buf).wait_send()
    out_local.wait()
    out_core.wait_send()
    b = out.at[orows]
    rcopy(b, b, tok_sem.at[2], out_sem.at[1], dc).wait_recv()


def local_fused(tokens, gate_weight, up_weight, down_weight, value_weight, glu_weight, out_weight, gate_scale, up_scale,
                down_scale, value_scale, glu_scale, out_scale, conv_kernel, norm_gain, first_gain, conv_gain, second_gain):
    F = lax.axis_size("fs")
    S, D = tokens.shape
    R, H = gate_weight.shape[0], gate_weight.shape[1] // 2
    C = value_weight.shape[1] // 2
    KW = conv_kernel.shape[0]
    RX = R // 2
    SH = S // 2
    y = lax.rem(lax.axis_index("fs"), 2)

    def part(array, side, dim):
        width = array.shape[dim] // 2
        return lax.dynamic_slice_in_dim(array, side * width, width, dim)

    def pack(side, *weights):
        cut = [part(w, side, 1).astype(jnp.bfloat16) for w in weights]
        whole = cut[0] if len(cut) == 1 else jnp.concatenate(cut, axis=1)
        return whole.reshape(2, RX, whole.shape[1])

    groups = ((gate_weight, up_weight), (down_weight,), (value_weight, glu_weight), (out_weight,))
    mine = [pack(y, *g) for g in groups]
    theirs = [pack(1 - y, *g) for g in groups]
    scales = jnp.zeros((8, R), jnp.float32).at[0].set(down_scale).at[1].set(out_scale)
    rows = [v.reshape(1, -1) for v in (first_gain, conv_gain, second_gain)]
    rows += [part(v, y, 0).reshape(1, -1) for v in (gate_scale, up_scale, value_scale, glu_scale, norm_gain)]
    taps = part(conv_kernel, y, 1)
    widths = [m.shape[2] for m in mine]
    G = len(groups)
    bf, f32 = jnp.bfloat16, jnp.float32
    dma = pltpu.SemaphoreType.DMA
    anyspace = pl.BlockSpec(memory_space=pl.ANY)
    vmem = pl.BlockSpec(memory_space=pltpu.VMEM)
    pad = -(-(KW - 1) // 8) * 8
    return pl.pallas_call(
        functools.partial(fused_kernel, (S, D, H, C, KW, F, RX)),
        out_shape=jax.ShapeDtypeStruct((S, D), bf),
        in_specs=[anyspace] * (2 + 2 * G) + [vmem] * 9,
        out_specs=anyspace,
        scratch_shapes=[pltpu.VMEM((2 * F, RX, w), bf) for w in widths]
        + [pltpu.VMEM((2, S, D), bf)] * 4
        + [pltpu.VMEM((2, S, H), bf), pltpu.VMEM((2, S, D), bf)]
        + [pltpu.VMEM((3, 2, SH, D), bf), pltpu.VMEM((3, SH, D), bf), pltpu.VMEM((3, SH, D), bf), pltpu.VMEM((3, SH, D), bf)]
        + [pltpu.VMEM((2, S + pad, C), f32), pltpu.VMEM((2, S, C), f32), pltpu.VMEM((2, S, C), bf)]
        + [pltpu.VMEM((4, 2, 8, S), f32), pltpu.VMEM((F, 8, R), f32), pltpu.VMEM((8, D), f32)]
        + [dma((G,)), dma((G, 2)), dma((G, 2)), dma((G, F)), dma((G, F)), dma((G, F)), dma((G, F)), dma((G, F))]
        + [dma((3,)), dma((F,)), dma((F,))]
        + [dma((3, 2)), dma((3, 2)), dma((3,)), dma((3,)), dma((2, 3)), dma((2, 3)), dma((3,)), dma((3,)), dma((4,))],
        compiler_params=pltpu.CompilerParams(
            collective_id=0, has_side_effects=True, vmem_limit_bytes=64 * 1024 * 1024 - 65536
        ),
    )(tokens, *mine, *theirs, scales, *rows, taps)


def rms_rows(rows, gains):
    values = rows.astype(jnp.float32)
    scaled = values * lax.rsqrt(jnp.mean(values * values, axis=-1, keepdims=True) + EPSILON)
    return (scaled * gains).astype(jnp.bfloat16)


def gated_hidden(normed, gate_full, up_full, gate_scale, up_scale):
    gate_part = jnp.dot(normed, gate_full, preferred_element_type=jnp.float32) * gate_scale
    upward = jnp.dot(normed, up_full, preferred_element_type=jnp.float32) * up_scale
    return (jax.nn.silu(gate_part) * upward).astype(jnp.bfloat16)


def causal_depthwise(inputs, kernel):
    taps = kernel.shape[0]
    length = inputs.shape[0]
    padded = jnp.concatenate(
        [jnp.zeros((taps - 1, inputs.shape[1]), jnp.float32), inputs.astype(jnp.float32)], axis=0
    )
    total = jnp.zeros((length, inputs.shape[1]), jnp.float32)
    for offset in range(taps):
        total = total + kernel[offset] * padded[offset : offset + length]
    return total


def swap(values, axis):
    return lax.ppermute(values, axis, [(0, 1), (1, 0)])


def gather_rows(rows, axis):
    if lax.axis_size(axis) != 2:
        return lax.all_gather(rows, axis, axis=0, tiled=True)
    other = swap(rows, axis)
    first = lax.axis_index(axis) == 0
    return jnp.concatenate([jnp.where(first, rows, other), jnp.where(first, other, rows)], axis=0)


def scatter_rows(partial, axis):
    members = lax.axis_size(axis)
    if members != 2:
        return lax.psum_scatter(partial, axis, scatter_dimension=0, tiled=True).astype(jnp.float32)
    own_rows = partial.shape[0] // members
    place = lax.axis_index(axis)
    mine = lax.dynamic_slice_in_dim(partial, place * own_rows, own_rows, 0)
    theirs = lax.dynamic_slice_in_dim(partial, (1 - place) * own_rows, own_rows, 0)
    return mine.astype(jnp.float32) + swap(theirs, axis).astype(jnp.float32)


def pull(rows, step):
    n = lax.axis_size("rep")
    return lax.ppermute(rows, "rep", [(s, (s - step) % n) for s in range(n)])


def push(rows, step):
    n = lax.axis_size("rep")
    return lax.ppermute(rows, "rep", [(s, (s + step) % n) for s in range(n)])


def streams_of(own):
    n = lax.axis_size("rep")
    parts = [own] + [pull(own, step) for step in range(1, n)]
    return [gather_rows(part, "tp") for part in parts]


def owned_sum(actives, weight_rows):
    n = lax.axis_size("rep")
    total = None
    for step in list(range(1, n)) + [0]:
        partial = lax.dot_general(
            actives[step], weight_rows, (((1,), (1,)), ((), ())), preferred_element_type=jnp.float32
        ).astype(jnp.bfloat16)
        part = scatter_rows(partial, "tp")
        if step:
            part = push(part.astype(jnp.bfloat16), step).astype(jnp.float32)
        total = part if total is None else total + part
    return total


def local_plain(
    tokens,
    gate_weight,
    up_weight,
    down_weight,
    value_weight,
    glu_weight,
    out_weight,
    gate_scale,
    up_scale,
    down_scale,
    value_scale,
    glu_scale,
    out_scale,
    conv_kernel,
    norm_gain,
    first_gain,
    conv_gain,
    second_gain,
):
    reps = lax.axis_size("rep")
    rep = lax.axis_index("rep")

    def part(array, dim):
        width = array.shape[dim] // reps
        return lax.dynamic_slice_in_dim(array, rep * width, width, dim)

    scales = lax.all_gather(jnp.stack([down_scale, out_scale]), "fs", axis=1, tiled=True)
    down_rows, out_rows = scales[0], scales[1]

    def full(weight):
        return lax.all_gather(part(weight, 1).astype(jnp.bfloat16), "fs", axis=0, tiled=True)

    gate_full, up_full, down_full, value_full, glu_full, out_full = (
        full(gate_weight),
        full(up_weight),
        full(down_weight),
        full(value_weight),
        full(glu_weight),
        full(out_weight),
    )
    gate_scale, up_scale, value_scale, glu_scale, norm_gain = (
        part(gate_scale, 0),
        part(up_scale, 0),
        part(value_scale, 0),
        part(glu_scale, 0),
        part(norm_gain, 0),
    )
    conv_kernel = part(conv_kernel, 1)
    members = lax.axis_size("tp")
    own_rows = tokens.shape[0] // members
    own_tokens = lax.dynamic_slice_in_dim(tokens, lax.axis_index("tp") * own_rows, own_rows, 0)

    normed = rms_rows(tokens, first_gain)
    own_normed = rms_rows(own_tokens, first_gain)
    rows = [normed] + [gather_rows(pull(own_normed, step), "tp") for step in range(1, reps)]
    hidden = [gated_hidden(r, gate_full, up_full, gate_scale, up_scale) for r in rows]
    after_first = (
        own_tokens.astype(jnp.float32) + 0.5 * down_rows * owned_sum(hidden, down_full)
    ).astype(jnp.bfloat16)
    mixes, sums = [], []
    for rows in streams_of(rms_rows(after_first, conv_gain)):
        value_part = jnp.dot(rows, value_full, preferred_element_type=jnp.float32) * value_scale
        gate_part = jnp.dot(rows, glu_full, preferred_element_type=jnp.float32) * glu_scale
        glu_in = (value_part * jax.nn.sigmoid(gate_part)).astype(jnp.bfloat16)
        mixed = causal_depthwise(glu_in, conv_kernel)
        mixes.append(mixed)
        sums.append(jnp.stack([jnp.sum(mixed, axis=1), jnp.sum(mixed * mixed, axis=1)]))
    totals = lax.psum(jnp.roll(jnp.stack(sums), rep, axis=0), ("rep", "tp"))
    totals = jnp.roll(totals, -rep, axis=0) / (norm_gain.shape[0] * reps * lax.axis_size("tp"))
    actives = []
    for step, mixed in enumerate(mixes):
        mean_rows = totals[step, 0][:, None]
        square_rows = totals[step, 1][:, None]
        normalized = (
            (mixed - mean_rows) * lax.rsqrt(square_rows - mean_rows * mean_rows + EPSILON) * norm_gain
        )
        actives.append(jax.nn.silu(normalized).astype(jnp.bfloat16))
    after_conv = (after_first.astype(jnp.float32) + out_rows * owned_sum(actives, out_full)).astype(
        jnp.bfloat16
    )
    hidden = [
        gated_hidden(r, gate_full, up_full, gate_scale, up_scale)
        for r in streams_of(rms_rows(after_conv, second_gain))
    ]
    after_second = (
        after_conv.astype(jnp.float32) + 0.5 * down_rows * owned_sum(hidden, down_full)
    ).astype(jnp.bfloat16)
    return gather_rows(after_second, "tp")


def fits(mesh):
    return mesh.shape["rep"] == 2 and mesh.shape["tp"] == 2 and mesh.shape["fs"] % 2 == 0 and mesh.shape["fs"] >= 4


def solution(mesh):
    columns, rows = P("fs", "tp"), P(("rep", "fs"), None)
    placed = (rows,) + (columns,) * 6 + (P("tp"), P("tp"), P("fs"), P("tp"), P("tp"), P("fs"), P(None, "tp"), P("tp"), P(), P(), P())
    local = local_fused if fits(mesh) else local_plain
    return jax.shard_map(local, mesh=mesh, in_specs=placed, out_specs=rows, check_vma=False)
```

```python
import functools

import jax
import jax.numpy as jnp
from jax import lax
from jax.experimental import pallas as pl
from jax.experimental.pallas import tpu as pltpu
from jax.sharding import PartitionSpec as P

MESH = pl.DeviceIdType.MESH
EPSILON = 1e-06
LANES = 128
TILE = 256
ROWS = 16
CHUNK = 32
SUBS = (1, 1, 1, 1)
COLS = 4
NT = (((1,), (1,)), ((), ()))
TN = (((0,), (0,)), ((), ()))


def fused_kernel(dims, *refs):
    S, D, H, C, KW, F, RX = dims
    Z = F // 2
    SH = S // 2
    R = 2 * RX
    PAD = -(-(KW - 1) // 8) * 8
    K, DC = SH // CHUNK, D // COLS
    (tokens, gate_w, up_w, down_w, value_w, glu_w, out_w, down_scale, out_scale, first_gain, conv_gain, second_gain,
     gate_scale, up_scale, value_scale, glu_scale, norm_gain, conv_k, out, *scratch) = refs
    (wb0, wb1, wb2, wb3, t0, t1, t2, t3, sg, tokv, xa, xb, xc, hid, part, rc, ry, ys, res, gp, mixed, act, st, sc, scl, dsc,
     f_sem, y_send, y_recv, u_send, d_send, z_recv, x_send, x_recv, tok_sem, s_send, s_recv,
     rc_send, rc_recv, ry_send, ry_recv, ag_send, ag_recv, fc_send, fc_recv, fy_send, fy_recv,
     st_send, st_recv, out_sem, oc_send, oc_recv) = scratch
    theirs, wb = (t0, t1, t2, t3), (wb0, wb1, wb2, wb3)
    G = len(wb)

    x = lax.axis_index("rep")
    f = lax.axis_index("fs")
    c = lax.axis_index("tp")
    y = lax.rem(f, 2)
    z = lax.div(f, 2)
    fp = f + 1 - 2 * y
    ox, oy, oc = 1 - x, 1 - y, 1 - c
    dx, dc, dy, dyc = {"rep": ox}, {"tp": oc}, {"fs": fp}, {"fs": fp, "tp": oc}
    up, dn = {"fs": f + 2}, {"fs": f - 2}

    def rcopy(src, dst, ssem, rsem, dev):
        return pltpu.make_async_remote_copy(
            src_ref=src, dst_ref=dst, send_sem=ssem, recv_sem=rsem, device_id=dev, device_id_type=MESH
        )

    def fetch(slot, ref, width, h, k):
        rows = pl.ds(h * RX, RX)
        return pltpu.make_async_copy(ref.at[rows], sg.at[slot, rows, pl.ds(0, width)], f_sem.at[slot, k])

    def fetch_start(slot, ref, width):
        for k, h in enumerate((x, ox)):
            fetch(slot, ref, width, h, k).start()

    def round_rows(g, off, slot, ref, width, k):
        h = (x, ox)[k]
        fetch(slot, ref, 2 * width, h, k).wait()

        @pl.loop(0, RX // ROWS)
        def _(i):
            rows = pl.ds(h * RX + i * ROWS, ROWS)
            r = pl.ds(i * ROWS, ROWS)
            near = sg[slot, rows, pl.ds(pl.multiple_of(y * width, LANES), width)]
            far = sg[slot, rows, pl.ds(pl.multiple_of(oy * width, LANES), width)]
            theirs[g][h, r, off:off + width] = far.astype(jnp.bfloat16)
            wb[g][2 * f + h, r, off:off + width] = near.astype(jnp.bfloat16)

    fetch_start(0, gate_w, 2 * H)
    fetch_start(1, up_w, 2 * H)
    tok_local = pltpu.make_async_copy(tokens, tokv.at[y], out_sem.at[0])
    tok_local.start()
    sc[...] = jnp.zeros_like(sc)
    sc[0:1, :] = down_scale[...]
    sc[1:2, :] = out_scale[...]

    barrier = pltpu.get_barrier_semaphore()
    for j in range(1, F):
        pl.semaphore_signal(barrier, inc=1, device_id={"fs": lax.rem(f + j, F)}, device_id_type=MESH)
    for dev in (dx, dc, dyc):
        pl.semaphore_signal(barrier, inc=1, device_id=dev, device_id_type=MESH)
    pl.semaphore_wait(barrier, F + 2)

    def piece(g, ref, lead, i):
        n = RX // SUBS[g]
        return ref.at[lead, pl.ds(i * n, n)]

    def y_copy(g, h, k, i):
        return rcopy(piece(g, theirs[g], h, i), piece(g, wb[g], 2 * f + h, i), y_send.at[g, k, i], y_recv.at[g, k, i], dy)

    def y_start(g, k):
        for i in range(SUBS[g]):
            y_copy(g, (x, ox)[k], k, i).start()

    def y_wait(g, h, k, i):
        b = piece(g, wb[g], 2 * fp + h, i)
        rcopy(b, b, y_send.at[g, k, i], y_recv.at[g, k, i], dy).wait_recv()

    def z_copy(g, q, i, sems, dev):
        b = piece(g, wb[g], 2 * q + x, i)
        return rcopy(b, b, sems.at[g, q, i], z_recv.at[g, q, i], dev)

    def x_copy(g, q, i):
        b = piece(g, wb[g], 2 * q + x, i)
        return rcopy(b, b, x_send.at[g, q, i], x_recv.at[g, q, i], dx)

    def send_rows(g, q, wait):
        for i in range(SUBS[g]):
            if wait:
                y_wait(g, x, 0, i)

            @pl.when(z < Z - 1)
            def _():
                z_copy(g, q, i, u_send, up).start()

            @pl.when(z > 0)
            def _():
                z_copy(g, q, i, d_send, dn).start()

    def forward(g, d):
        for k in range(2):
            yy = y if k == 0 else oy
            for i in range(SUBS[g]):
                @pl.when(z >= d)
                def _():
                    q = 2 * (z - d) + yy
                    z_copy(g, q, i, u_send, up).wait_recv()

                    @pl.when(z < Z - 1)
                    def _():
                        z_copy(g, q, i, u_send, up).start()

                    x_copy(g, q, i).start()

                @pl.when(z + d < Z)
                def _():
                    q = 2 * (z + d) + yy
                    z_copy(g, q, i, d_send, dn).wait_recv()

                    @pl.when(z > 0)
                    def _():
                        z_copy(g, q, i, d_send, dn).start()

                    x_copy(g, q, i).start()

    def group_done(g):
        for i in range(SUBS[g]):
            y_wait(g, ox, 1, i)

        @pl.loop(0, F)
        def _(q):
            @pl.when(lax.div(q, 2) != z)
            def _():
                for i in range(SUBS[g]):
                    b = piece(g, wb[g], 2 * q + ox, i)
                    rcopy(b, b, x_send.at[g, q, i], x_recv.at[g, q, i], dx).wait_recv()

    def drain(g):
        for k, h in enumerate((x, ox)):
            for i in range(SUBS[g]):
                y_copy(g, h, k, i).wait_send()

        @pl.loop(0, F)
        def _(q):
            zq = lax.div(q, 2)

            @pl.when((z < Z - 1) & (zq <= z))
            def _():
                for i in range(SUBS[g]):
                    z_copy(g, q, i, u_send, up).wait_send()

            @pl.when((z > 0) & (zq >= z))
            def _():
                for i in range(SUBS[g]):
                    z_copy(g, q, i, d_send, dn).wait_send()

            @pl.when(zq != z)
            def _():
                for i in range(SUBS[g]):
                    x_copy(g, q, i).wait_send()

    for k in range(2):
        round_rows(0, 0, 0, gate_w, H, k)
        round_rows(0, H, 1, up_w, H, k)
    y_start(0, 0)
    send_rows(0, f, False)
    fetch_start(0, down_w, 2 * H)
    fetch_start(1, value_w, 2 * C)
    for k in range(2):
        round_rows(1, 0, 0, down_w, H, k)
    fetch_start(0, glu_w, 2 * C)
    y_start(1, 0)
    for k in range(2):
        round_rows(2, 0, 1, value_w, C, k)
    fetch_start(1, out_w, 2 * C)
    for k in range(2):
        round_rows(2, C, 0, glu_w, C, k)
    y_start(2, 0)
    for k in range(2):
        round_rows(3, 0, 1, out_w, C, k)
    y_start(3, 0)
    y_start(0, 1)
    tok_y = rcopy(tokens, tokv.at[y], tok_sem.at[0], tok_sem.at[1], dy)
    tok_y.start()
    for g in range(1, G):
        y_start(g, 1)
    for j in range(1, F):
        rcopy(sc, scl.at[f], s_send.at[j], s_recv.at[f], {"fs": lax.rem(f + j, F)}).start()

    def norm(v, gains):
        return (v * lax.rsqrt(jnp.mean(v * v, axis=-1, keepdims=True) + EPSILON) * gains).astype(jnp.bfloat16)

    def norm_tokens(s):
        @pl.loop(0, S // ROWS)
        def _(i):
            r = pl.ds(i * ROWS, ROWS)
            xa[s, r, :] = norm(tokv[s, r, :].astype(jnp.float32), first_gain[...])

    def gate_up(src, s):
        @pl.loop(0, H // TILE)
        def _(j):
            lo = pl.multiple_of(j * TILE, TILE)
            a = src[s]
            gw = wb0[:, :, pl.ds(lo, TILE)].reshape(D, TILE)
            uw = wb0[:, :, pl.ds(H + lo, TILE)].reshape(D, TILE)
            gv = jnp.dot(a, gw, preferred_element_type=jnp.float32) * gate_scale[:, pl.ds(pl.multiple_of(y * H + lo, LANES), TILE)]
            uv = jnp.dot(a, uw, preferred_element_type=jnp.float32) * up_scale[:, pl.ds(pl.multiple_of(y * H + lo, LANES), TILE)]
            hid[s, :, pl.ds(lo, TILE)] = (gv * jax.nn.sigmoid(gv) * uv).astype(jnp.bfloat16)

    def project(src, w, width, s, first=0, last=F):
        @pl.loop(first, last)
        def _(j):
            rows = w[pl.ds(2 * j, 2)].reshape(R, width)
            p = lax.dot_general(src[s], rows, NT, preferred_element_type=jnp.float32)
            part[s, :, pl.ds(pl.multiple_of(j * R, R), R)] = p.astype(jnp.bfloat16)

    crows = pl.ds(c * SH, SH)
    orows = pl.ds(oc * SH, SH)

    def rs_core(u, s):
        return rcopy(part.at[s, orows], rc.at[u, s], rc_send.at[u, s], rc_recv.at[u, s], dc)

    def rs_pair(u, k):
        r = pl.ds(k * CHUNK, CHUNK)
        return rcopy(ys.at[u, r], ry.at[u, r], ry_send.at[u, k], ry_recv.at[u, k], dy)

    def rs_push(u):
        rs_core(u, oy).wait_recv()
        for k in range(K):
            @pl.loop(0, CHUNK // ROWS)
            def _(i):
                r = pl.ds(k * CHUNK + i * ROWS, ROWS)
                p = part[oy, pl.ds(c * SH + k * CHUNK + i * ROWS, ROWS), :].astype(jnp.float32)
                ys[u, r, :] = (p + rc[u, oy, r, :].astype(jnp.float32)).astype(jnp.bfloat16)

            rs_pair(u, k).start()

    def rs_finish(u, base, factor, scale_row, gains, dst):
        rs_core(u, y).wait_recv()
        for k in range(K):
            rs_pair(u, k).wait_recv()

            @pl.loop(0, CHUNK // ROWS)
            def _(i):
                r = pl.ds(k * CHUNK + i * ROWS, ROWS)
                rr = pl.ds(c * SH + k * CHUNK + i * ROWS, ROWS)
                total = part[y, rr, :].astype(jnp.float32) + rc[u, y, r, :].astype(jnp.float32)
                total = total + ry[u, r, :].astype(jnp.float32)
                b = tokv[y, rr, :] if base is None else res[base, r, :]
                now = (b.astype(jnp.float32) + dsc[scale_row:scale_row + 1, :] * factor * total).astype(jnp.bfloat16)
                res[u, r, :] = now
                dst[y, rr, :] = norm(now.astype(jnp.float32), gains[...])

            ag_copy(u, 1, k, dst).start()
            ag_copy(u, 0, k, dst).start()

    def ag_rows(k, side):
        return pl.ds(side * SH + k * CHUNK, CHUNK)

    def ag_copy(u, kind, k, buf):
        b = buf.at[oy if kind == 2 else y, ag_rows(k, c)]
        return rcopy(b, b, ag_send.at[u, kind, k], ag_recv.at[u, kind, k], dy if kind == 1 else dc)

    def ag_wait(u, kind, k, buf):
        b = buf.at[y if kind == 0 else oy, ag_rows(k, c if kind == 1 else oc)]
        rcopy(b, b, ag_send.at[u, kind, k], ag_recv.at[u, kind, k], dc).wait_recv()

    def ag_pass(u, buf, first, last):
        for k in range(first, last):
            ag_wait(u, 1, k, buf)
            ag_copy(u, 2, k, buf).start()

    def ag_own(u, buf):
        for k in range(K):
            ag_wait(u, 0, k, buf)

    def ag_other(u, buf):
        for k in range(K):
            ag_wait(u, 2, k, buf)

    def fc_copy(s, q):
        cols = pl.ds(q * DC, DC)
        return rcopy(part.at[s, orows, cols], rc.at[2, s, :, cols], fc_send.at[s, q], fc_recv.at[s, q], dc)

    def fy_copy(q):
        cols = pl.ds(q * DC, DC)
        return rcopy(ys.at[2, :, cols], ry.at[2, :, cols], fy_send.at[q], fy_recv.at[q], dy)

    def last_push(q):
        cols = pl.ds(q * DC, DC)
        fc_copy(oy, q).wait_recv()

        @pl.loop(0, SH // ROWS)
        def _(i):
            r = pl.ds(i * ROWS, ROWS)
            p = part[oy, pl.ds(c * SH + i * ROWS, ROWS), cols].astype(jnp.float32)
            ys[2, r, cols] = (p + rc[2, oy, r, cols].astype(jnp.float32)).astype(jnp.bfloat16)

        fy_copy(q).start()

    def out_copies(q):
        cols = pl.ds(q * DC, DC)
        src, dst = res.at[2, :, cols], out.at[crows, cols]
        return pltpu.make_async_copy(src, dst, out_sem.at[q]), rcopy(src, dst, oc_send.at[q], oc_recv.at[q], dc)

    def last_finish(q):
        cols = pl.ds(q * DC, DC)
        fc_copy(y, q).wait_recv()
        fy_copy(q).wait_recv()

        @pl.loop(0, SH // ROWS)
        def _(i):
            r = pl.ds(i * ROWS, ROWS)
            total = part[y, pl.ds(c * SH + i * ROWS, ROWS), cols].astype(jnp.float32) + rc[2, y, r, cols].astype(jnp.float32)
            total = total + ry[2, r, cols].astype(jnp.float32)
            res[2, r, cols] = (res[1, r, cols].astype(jnp.float32) + 0.5 * dsc[0:1, cols] * total).astype(jnp.bfloat16)

        for cp in out_copies(q):
            cp.start()

    def value_glu(s):
        @pl.loop(0, C // TILE)
        def _(j):
            lo = pl.multiple_of(j * TILE, TILE)
            a = xb[s]
            vw = wb2[:, :, pl.ds(lo, TILE)].reshape(D, TILE)
            gw = wb2[:, :, pl.ds(C + lo, TILE)].reshape(D, TILE)
            vv = jnp.dot(a, vw, preferred_element_type=jnp.float32) * value_scale[:, pl.ds(pl.multiple_of(y * C + lo, LANES), TILE)]
            gv = jnp.dot(a, gw, preferred_element_type=jnp.float32) * glu_scale[:, pl.ds(pl.multiple_of(y * C + lo, LANES), TILE)]
            g = (vv * jax.nn.sigmoid(gv)).astype(jnp.bfloat16)
            gp[s, pl.ds(PAD, S), pl.ds(lo, TILE)] = g.astype(jnp.float32)

    def convolve(s):
        @pl.loop(0, C // LANES)
        def _(j):
            cols = pl.ds(pl.multiple_of(j * LANES, LANES), LANES)
            near = pl.ds(pl.multiple_of(y * C + j * LANES, LANES), LANES)
            gp[s, pl.ds(0, PAD), cols] = jnp.zeros((PAD, LANES), jnp.float32)
            total = jnp.zeros((S, LANES), jnp.float32)
            for k in range(KW):
                total = total + conv_k[k:k + 1, near] * gp[s, pl.ds(PAD - (KW - 1) + k, S), cols]
            mixed[s, :, cols] = total

        m = mixed[s]
        low = lax.broadcasted_iota(jnp.int32, (8, C), 0) < 4
        one, nil = jnp.ones((8, C), jnp.float32), jnp.zeros((8, C), jnp.float32)
        hi = lax.Precision.HIGHEST
        sums = lax.dot_general(jnp.where(low, one, nil), m, NT, precision=hi, preferred_element_type=jnp.float32)
        squares = lax.dot_general(jnp.where(low, nil, one), m * m, NT, precision=hi, preferred_element_type=jnp.float32)
        st[0, s] = sums + squares

    def st_copies():
        return [rcopy(st.at[0], st.at[k + 1], st_send.at[k], st_recv.at[k], dev) for k, dev in enumerate((dc, dy, dyc))]

    def activate(s):
        total = st[0, s] + st[1, s] + st[2, s] + st[3, s]
        total = total / D
        mean, square = total[0:1], total[4:5]
        rstd = lax.rsqrt(square - mean * mean + EPSILON)
        row = lax.broadcasted_iota(jnp.int32, (8, S), 0)
        both = jnp.where(row == 0, jnp.broadcast_to(mean, (8, S)), jnp.where(row == 1, jnp.broadcast_to(rstd, (8, S)), 0.0))
        pick = lax.broadcasted_iota(jnp.int32, (8, LANES), 0)
        hi = lax.Precision.HIGHEST
        mcol = lax.dot_general(both, jnp.where(pick == 0, 1.0, 0.0), TN, precision=hi, preferred_element_type=jnp.float32)
        rcol = lax.dot_general(both, jnp.where(pick == 1, 1.0, 0.0), TN, precision=hi, preferred_element_type=jnp.float32)
        for j in range(C // LANES):
            cols = slice(j * LANES, (j + 1) * LANES)
            v = (mixed[s, :, cols] - mcol) * rcol * norm_gain[:, pl.ds(pl.multiple_of(y * C + j * LANES, LANES), LANES)]
            act[s, :, cols] = (v * jax.nn.sigmoid(v)).astype(jnp.bfloat16)

    def own_and_pair(g):
        send_rows(g, f, False)
        send_rows(g, fp, True)

    send_rows(0, fp, True)
    tok_local.wait()
    norm_tokens(y)
    forward(0, 1)
    for d in range(2, Z - 1):
        forward(0, d)
    own_and_pair(1)
    tok_y.wait_recv()
    norm_tokens(oy)
    forward(0, Z - 1)
    forward(1, 1)
    group_done(0)
    gate_up(xa, oy)
    for d in range(2, Z - 1):
        forward(1, d)
    own_and_pair(2)
    gate_up(xa, y)
    forward(1, Z - 1)
    forward(2, 1)
    group_done(1)
    project(hid, wb1, H, oy)
    rs_core(0, oy).start()
    project(hid, wb1, H, y)
    rs_core(0, y).start()
    rs_push(0)
    for j in range(1, F):
        b = scl.at[lax.rem(f + j, F)]
        rcopy(b, b, s_send.at[j], s_recv.at[lax.rem(f + j, F)], dy).wait_recv()
    scl[f] = sc[...]
    for j in range(F):
        dsc[:, j * R:(j + 1) * R] = scl[j]
    for d in range(2, Z - 1):
        forward(2, d)
    own_and_pair(3)
    forward(2, Z - 1)
    forward(3, 1)
    rs_finish(0, None, 0.5, 0, conv_gain, xb)
    for d in range(2, Z):
        forward(3, d)
    ag_pass(0, xb, 0, K)
    ag_own(0, xb)
    group_done(2)
    value_glu(y)
    convolve(y)
    ag_other(0, xb)
    value_glu(oy)
    convolve(oy)
    for cp in st_copies():
        cp.start()
    for s in range(2):
        rs_core(0, s).wait_send()
    for cp in st_copies():
        cp.wait()
    group_done(3)
    activate(oy)
    project(act, wb3, C, oy)
    rs_core(1, oy).start()
    activate(y)
    project(act, wb3, C, y)
    rs_core(1, y).start()
    rs_push(1)
    for g in range(G):
        drain(g)
    rs_finish(1, 0, 1.0, 1, second_gain, xc)
    ag_own(1, xc)
    gate_up(xc, y)
    for s in range(2):
        rs_core(1, s).wait_send()
    ag_pass(1, xc, 0, K)
    ag_other(1, xc)
    gate_up(xc, oy)
    step = F // COLS
    for q in range(COLS):
        project(hid, wb1, H, oy, q * step, (q + 1) * step)
        fc_copy(oy, q).start()
        if q:
            last_push(q - 1)
    for q in range(COLS):
        project(hid, wb1, H, y, q * step, (q + 1) * step)
        fc_copy(y, q).start()
        if q == 0:
            last_push(COLS - 1)
    tok_y.wait_send()
    for j in range(1, F):
        rcopy(sc, scl.at[f], s_send.at[j], s_recv.at[f], dy).wait_send()
    for u, buf in enumerate((xb, xc)):
        for k in range(K):
            rs_pair(u, k).wait_send()
            for kind in range(3):
                ag_copy(u, kind, k, buf).wait_send()
    for q in range(COLS):
        last_finish(q)
    for q in range(COLS):
        for s in range(2):
            fc_copy(s, q).wait_send()
        fy_copy(q).wait_send()
        near, far = out_copies(q)
        near.wait()
        far.wait_send()
        b = out.at[orows, pl.ds(q * DC, DC)]
        rcopy(b, b, oc_send.at[q], oc_recv.at[q], dc).wait_recv()


def local_fused(tokens, gate_weight, up_weight, down_weight, value_weight, glu_weight, out_weight, gate_scale, up_scale,
                down_scale, value_scale, glu_scale, out_scale, conv_kernel, norm_gain, first_gain, conv_gain, second_gain):
    F = lax.axis_size("fs")
    S, D = tokens.shape
    R, H = gate_weight.shape[0], gate_weight.shape[1] // 2
    C = value_weight.shape[1] // 2
    KW = conv_kernel.shape[0]
    RX = R // 2
    SH = S // 2
    vectors = (down_scale, out_scale, first_gain, conv_gain, second_gain, gate_scale, up_scale, value_scale, glu_scale, norm_gain)
    rows = [v.reshape(1, -1) for v in vectors]
    widths = (2 * H, H, 2 * C, C)
    G, K, NS = len(widths), SH // CHUNK, max(SUBS)
    bf, f32 = jnp.bfloat16, jnp.float32
    dma = pltpu.SemaphoreType.DMA
    anyspace = pl.BlockSpec(memory_space=pl.ANY)
    vmem = pl.BlockSpec(memory_space=pltpu.VMEM)
    pad = -(-(KW - 1) // 8) * 8
    return pl.pallas_call(
        functools.partial(fused_kernel, (S, D, H, C, KW, F, RX)),
        out_shape=jax.ShapeDtypeStruct((S, D), bf),
        in_specs=[anyspace] * 7 + [vmem] * 11,
        out_specs=anyspace,
        scratch_shapes=[pltpu.VMEM((2 * F, RX, w), bf) for w in widths]
        + [pltpu.VMEM((2, RX, w), bf) for w in widths]
        + [pltpu.VMEM((2, R, 2 * H), f32)]
        + [pltpu.VMEM((2, S, D), bf)] * 4
        + [pltpu.VMEM((2, S, H), bf), pltpu.VMEM((2, S, D), bf)]
        + [pltpu.VMEM((3, 2, SH, D), bf), pltpu.VMEM((3, SH, D), bf), pltpu.VMEM((3, SH, D), bf), pltpu.VMEM((3, SH, D), bf)]
        + [pltpu.VMEM((2, S + pad, C), f32), pltpu.VMEM((2, S, C), f32), pltpu.VMEM((2, S, C), bf)]
        + [pltpu.VMEM((4, 2, 8, S), f32), pltpu.VMEM((8, R), f32), pltpu.VMEM((F, 8, R), f32), pltpu.VMEM((8, D), f32)]
        + [dma((2, 2)), dma((G, 2, NS)), dma((G, 2, NS))] + [dma((G, F, NS))] * 5
        + [dma((2,)), dma((F,)), dma((F,))]
        + [dma((3, 2)), dma((3, 2)), dma((2, K)), dma((2, K)), dma((2, 3, K)), dma((2, 3, K))]
        + [dma((2, COLS)), dma((2, COLS)), dma((COLS,)), dma((COLS,))]
        + [dma((3,)), dma((3,)), dma((COLS,)), dma((COLS,)), dma((COLS,))],
        compiler_params=pltpu.CompilerParams(
            collective_id=0, has_side_effects=True, vmem_limit_bytes=64 * 1024 * 1024 - 65536
        ),
    )(tokens, gate_weight, up_weight, down_weight, value_weight, glu_weight, out_weight, *rows, conv_kernel)


def rms_rows(rows, gains):
    values = rows.astype(jnp.float32)
    scaled = values * lax.rsqrt(jnp.mean(values * values, axis=-1, keepdims=True) + EPSILON)
    return (scaled * gains).astype(jnp.bfloat16)


def gated_hidden(normed, gate_full, up_full, gate_scale, up_scale):
    gate_part = jnp.dot(normed, gate_full, preferred_element_type=jnp.float32) * gate_scale
    upward = jnp.dot(normed, up_full, preferred_element_type=jnp.float32) * up_scale
    return (jax.nn.silu(gate_part) * upward).astype(jnp.bfloat16)


def causal_depthwise(inputs, kernel):
    taps = kernel.shape[0]
    length = inputs.shape[0]
    padded = jnp.concatenate(
        [jnp.zeros((taps - 1, inputs.shape[1]), jnp.float32), inputs.astype(jnp.float32)], axis=0
    )
    total = jnp.zeros((length, inputs.shape[1]), jnp.float32)
    for offset in range(taps):
        total = total + kernel[offset] * padded[offset : offset + length]
    return total


def swap(values, axis):
    return lax.ppermute(values, axis, [(0, 1), (1, 0)])


def gather_rows(rows, axis):
    if lax.axis_size(axis) != 2:
        return lax.all_gather(rows, axis, axis=0, tiled=True)
    other = swap(rows, axis)
    first = lax.axis_index(axis) == 0
    return jnp.concatenate([jnp.where(first, rows, other), jnp.where(first, other, rows)], axis=0)


def scatter_rows(partial, axis):
    members = lax.axis_size(axis)
    if members != 2:
        return lax.psum_scatter(partial, axis, scatter_dimension=0, tiled=True).astype(jnp.float32)
    own_rows = partial.shape[0] // members
    place = lax.axis_index(axis)
    mine = lax.dynamic_slice_in_dim(partial, place * own_rows, own_rows, 0)
    theirs = lax.dynamic_slice_in_dim(partial, (1 - place) * own_rows, own_rows, 0)
    return mine.astype(jnp.float32) + swap(theirs, axis).astype(jnp.float32)


def pull(rows, step):
    n = lax.axis_size("rep")
    return lax.ppermute(rows, "rep", [(s, (s - step) % n) for s in range(n)])


def push(rows, step):
    n = lax.axis_size("rep")
    return lax.ppermute(rows, "rep", [(s, (s + step) % n) for s in range(n)])


def streams_of(own):
    n = lax.axis_size("rep")
    parts = [own] + [pull(own, step) for step in range(1, n)]
    return [gather_rows(part, "tp") for part in parts]


def owned_sum(actives, weight_rows):
    n = lax.axis_size("rep")
    total = None
    for step in list(range(1, n)) + [0]:
        partial = lax.dot_general(
            actives[step], weight_rows, (((1,), (1,)), ((), ())), preferred_element_type=jnp.float32
        ).astype(jnp.bfloat16)
        part = scatter_rows(partial, "tp")
        if step:
            part = push(part.astype(jnp.bfloat16), step).astype(jnp.float32)
        total = part if total is None else total + part
    return total


def local_plain(
    tokens,
    gate_weight,
    up_weight,
    down_weight,
    value_weight,
    glu_weight,
    out_weight,
    gate_scale,
    up_scale,
    down_scale,
    value_scale,
    glu_scale,
    out_scale,
    conv_kernel,
    norm_gain,
    first_gain,
    conv_gain,
    second_gain,
):
    reps = lax.axis_size("rep")
    rep = lax.axis_index("rep")

    def part(array, dim):
        width = array.shape[dim] // reps
        return lax.dynamic_slice_in_dim(array, rep * width, width, dim)

    scales = lax.all_gather(jnp.stack([down_scale, out_scale]), "fs", axis=1, tiled=True)
    down_rows, out_rows = scales[0], scales[1]

    def full(weight):
        return lax.all_gather(part(weight, 1).astype(jnp.bfloat16), "fs", axis=0, tiled=True)

    gate_full, up_full, down_full, value_full, glu_full, out_full = (
        full(gate_weight),
        full(up_weight),
        full(down_weight),
        full(value_weight),
        full(glu_weight),
        full(out_weight),
    )
    gate_scale, up_scale, value_scale, glu_scale, norm_gain = (
        part(gate_scale, 0),
        part(up_scale, 0),
        part(value_scale, 0),
        part(glu_scale, 0),
        part(norm_gain, 0),
    )
    conv_kernel = part(conv_kernel, 1)
    members = lax.axis_size("tp")
    own_rows = tokens.shape[0] // members
    own_tokens = lax.dynamic_slice_in_dim(tokens, lax.axis_index("tp") * own_rows, own_rows, 0)

    normed = rms_rows(tokens, first_gain)
    own_normed = rms_rows(own_tokens, first_gain)
    rows = [normed] + [gather_rows(pull(own_normed, step), "tp") for step in range(1, reps)]
    hidden = [gated_hidden(r, gate_full, up_full, gate_scale, up_scale) for r in rows]
    after_first = (
        own_tokens.astype(jnp.float32) + 0.5 * down_rows * owned_sum(hidden, down_full)
    ).astype(jnp.bfloat16)
    mixes, sums = [], []
    for rows in streams_of(rms_rows(after_first, conv_gain)):
        value_part = jnp.dot(rows, value_full, preferred_element_type=jnp.float32) * value_scale
        gate_part = jnp.dot(rows, glu_full, preferred_element_type=jnp.float32) * glu_scale
        glu_in = (value_part * jax.nn.sigmoid(gate_part)).astype(jnp.bfloat16)
        mixed = causal_depthwise(glu_in, conv_kernel)
        mixes.append(mixed)
        sums.append(jnp.stack([jnp.sum(mixed, axis=1), jnp.sum(mixed * mixed, axis=1)]))
    totals = lax.psum(jnp.roll(jnp.stack(sums), rep, axis=0), ("rep", "tp"))
    totals = jnp.roll(totals, -rep, axis=0) / (norm_gain.shape[0] * reps * lax.axis_size("tp"))
    actives = []
    for step, mixed in enumerate(mixes):
        mean_rows = totals[step, 0][:, None]
        square_rows = totals[step, 1][:, None]
        normalized = (
            (mixed - mean_rows) * lax.rsqrt(square_rows - mean_rows * mean_rows + EPSILON) * norm_gain
        )
        actives.append(jax.nn.silu(normalized).astype(jnp.bfloat16))
    after_conv = (after_first.astype(jnp.float32) + out_rows * owned_sum(actives, out_full)).astype(
        jnp.bfloat16
    )
    hidden = [
        gated_hidden(r, gate_full, up_full, gate_scale, up_scale)
        for r in streams_of(rms_rows(after_conv, second_gain))
    ]
    after_second = (
        after_conv.astype(jnp.float32) + 0.5 * down_rows * owned_sum(hidden, down_full)
    ).astype(jnp.bfloat16)
    return gather_rows(after_second, "tp")


def fits(mesh):
    return mesh.shape["rep"] == 2 and mesh.shape["tp"] == 2 and mesh.shape["fs"] % 2 == 0 and mesh.shape["fs"] >= 4


def solution(mesh):
    columns, rows = P("fs", "tp"), P(("rep", "fs"), None)
    placed = (rows,) + (columns,) * 6 + (P("tp"), P("tp"), P("fs"), P("tp"), P("tp"), P("fs"), P(None, "tp"), P("tp"), P(), P(), P())
    local = local_fused if fits(mesh) else local_plain
    return jax.shard_map(local, mesh=mesh, in_specs=placed, out_specs=rows, check_vma=False)
```

```python
import functools

import jax
import jax.numpy as jnp
from jax import lax
from jax.experimental import pallas as pl
from jax.experimental.pallas import tpu as pltpu
from jax.sharding import PartitionSpec as P

MESH = pl.DeviceIdType.MESH
EPSILON = 1e-06
LANES = 128
TILE = 256
ROWS = 16
CHUNK = 32
SUBS = (2, 1, 1, 1)
VIA_X = ((0, 1), (0, 2), (0, 3))
COLS = 4
NT = (((1,), (1,)), ((), ()))
TN = (((0,), (0,)), ((), ()))


def fused_kernel(dims, *refs):
    S, D, H, C, KW, F, RX = dims
    Z = F // 2
    SH = S // 2
    R = 2 * RX
    PAD = -(-(KW - 1) // 8) * 8
    K, DC = SH // CHUNK, D // COLS
    (tokens, gate_w, up_w, down_w, value_w, glu_w, out_w, down_scale, out_scale, first_gain, conv_gain, second_gain,
     gate_scale, up_scale, value_scale, glu_scale, norm_gain, conv_k, out, *scratch) = refs
    (wb0, wb1, wb2, wb3, t0, t1, t2, t3, sg, tokv, xa, xb, xc, hid, part, rc, ry, ys, res, gp, mixed, act, st, sc, scl, dsc,
     f_sem, y_send, y_recv, u_send, d_send, t_send, z_recv, x_send, x_recv, tok_sem, s_send, s_recv,
     rc_send, rc_recv, ry_send, ry_recv, ag_send, ag_recv, fc_send, fc_recv, fy_send, fy_recv,
     st_send, st_recv, out_sem, oc_send, oc_recv) = scratch
    theirs, wb = (t0, t1, t2, t3), (wb0, wb1, wb2, wb3)
    G = len(wb)

    x = lax.axis_index("rep")
    f = lax.axis_index("fs")
    c = lax.axis_index("tp")
    y = lax.rem(f, 2)
    z = lax.div(f, 2)
    fp = f + 1 - 2 * y
    ox, oy, oc = 1 - x, 1 - y, 1 - c
    a = lax.rem(z, 2)
    oa = 1 - a
    dx, dc, dy, dyc = {"rep": ox}, {"tp": oc}, {"fs": fp}, {"fs": fp, "tp": oc}
    dz = {"fs": f + 2 - 4 * a}
    up, dn = {"fs": f + 2}, {"fs": f - 2}
    up2, dn2 = {"fs": f + 4}, {"fs": f - 4}

    def rcopy(src, dst, ssem, rsem, dev):
        return pltpu.make_async_remote_copy(
            src_ref=src, dst_ref=dst, send_sem=ssem, recv_sem=rsem, device_id=dev, device_id_type=MESH
        )

    def fetch(slot, ref, width, h, k):
        rows = pl.ds(h * RX, RX)
        return pltpu.make_async_copy(ref.at[rows], sg.at[slot, rows, pl.ds(0, width)], f_sem.at[slot, k])

    def fetch_start(slot, ref, width):
        for k, h in enumerate((x, ox)):
            fetch(slot, ref, width, h, k).start()

    def round_rows(g, off, slot, ref, width, k):
        h = (x, ox)[k]
        side = a if g < 2 else y
        fetch(slot, ref, 2 * width, h, k).wait()

        @pl.loop(0, RX // ROWS)
        def _(i):
            rows = pl.ds(h * RX + i * ROWS, ROWS)
            r = pl.ds(i * ROWS, ROWS)
            near = sg[slot, rows, pl.ds(pl.multiple_of(side * width, LANES), width)]
            wb[g][2 * f + h, r, off:off + width] = near.astype(jnp.bfloat16)
            if g >= 2 or k == 0:
                far = sg[slot, rows, pl.ds(pl.multiple_of((1 - side) * width, LANES), width)]
                theirs[g][h if g >= 2 else 0, r, off:off + width] = far.astype(jnp.bfloat16)

    fetch_start(0, gate_w, 2 * H)
    fetch_start(1, up_w, 2 * H)
    tok_local = pltpu.make_async_copy(tokens, tokv.at[a], out_sem.at[0])
    tok_local.start()
    sc[...] = jnp.zeros_like(sc)
    sc[0:1, :] = down_scale[...]
    sc[1:2, :] = out_scale[...]

    barrier = pltpu.get_barrier_semaphore()
    for j in range(1, F):
        pl.semaphore_signal(barrier, inc=1, device_id={"fs": lax.rem(f + j, F)}, device_id_type=MESH)
    for dev in (dx, dc, dyc):
        pl.semaphore_signal(barrier, inc=1, device_id=dev, device_id_type=MESH)
    pl.semaphore_wait(barrier, F + 2)

    def piece(g, ref, lead, i):
        n = RX // SUBS[g]
        return ref.at[lead, pl.ds(i * n, n)]

    def y_copy(g, h, k, i):
        return rcopy(piece(g, theirs[g], h, i), piece(g, wb[g], 2 * f + h, i), y_send.at[g, 0, k, i], y_recv.at[g, 0, k, i], dy)

    def y_start(g, k):
        for i in range(SUBS[g]):
            y_copy(g, (x, ox)[k], k, i).start()

    def y_wait(g, h, k, i):
        b = piece(g, wb[g], 2 * fp + h, i)
        rcopy(b, b, y_send.at[g, 0, k, i], y_recv.at[g, 0, k, i], dy).wait_recv()

    def z_copy(g, q, i, sems, dev):
        b = piece(g, wb[g], 2 * q + x, i)
        return rcopy(b, b, sems.at[g, q, i], z_recv.at[g, q, i], dev)

    def x_copy(g, q, i):
        b = piece(g, wb[g], 2 * q + x, i)
        return rcopy(b, b, x_send.at[g, q, i], x_recv.at[g, q, i], dx)

    def send_rows(g, q, wait):
        for i in range(SUBS[g]):
            if wait:
                y_wait(g, x, 0, i)

            @pl.when(z < Z - 1)
            def _():
                z_copy(g, q, i, u_send, up).start()

            @pl.when(z > 0)
            def _():
                z_copy(g, q, i, d_send, dn).start()

    def forward(g, d):
        for k in range(2):
            yy = y if k == 0 else oy
            for i in range(SUBS[g]):
                @pl.when(z >= d)
                def _():
                    q = 2 * (z - d) + yy
                    z_copy(g, q, i, u_send, up).wait_recv()

                    @pl.when(z < Z - 1)
                    def _():
                        z_copy(g, q, i, u_send, up).start()

                    x_copy(g, q, i).start()

                @pl.when(z + d < Z)
                def _():
                    q = 2 * (z + d) + yy
                    z_copy(g, q, i, d_send, dn).wait_recv()

                    @pl.when(z > 0)
                    def _():
                        z_copy(g, q, i, d_send, dn).start()

                    x_copy(g, q, i).start()

    def group_done(g):
        for i in range(SUBS[g]):
            y_wait(g, ox, 1, i)

        @pl.loop(0, F)
        def _(q):
            @pl.when(lax.div(q, 2) != z)
            def _():
                for i in range(SUBS[g]):
                    b = piece(g, wb[g], 2 * q + ox, i)
                    rcopy(b, b, x_send.at[g, q, i], x_recv.at[g, q, i], dx).wait_recv()

    def drain(g):
        for k, h in enumerate((x, ox)):
            for i in range(SUBS[g]):
                y_copy(g, h, k, i).wait_send()

        @pl.loop(0, F)
        def _(q):
            zq = lax.div(q, 2)

            @pl.when((z < Z - 1) & (zq <= z))
            def _():
                for i in range(SUBS[g]):
                    z_copy(g, q, i, u_send, up).wait_send()

            @pl.when((z > 0) & (zq >= z))
            def _():
                for i in range(SUBS[g]):
                    z_copy(g, q, i, d_send, dn).wait_send()

            @pl.when(zq != z)
            def _():
                for i in range(SUBS[g]):
                    x_copy(g, q, i).wait_send()

    def ff_own(g):
        for i in range(SUBS[g]):
            b = piece(g, wb[g], 2 * f + x, i)
            t = piece(g, theirs[g], 0, i)

            @pl.when(z > 0)
            def _():
                rcopy(t, b, t_send.at[g, 0, i], z_recv.at[g, f, i], dn).start()

            @pl.when(z < Z - 1)
            def _():
                rcopy(t, b, t_send.at[g, 1, i], z_recv.at[g, f, i], up).start()

            @pl.when(z >= 2)
            def _():
                z_copy(g, f, i, d_send, dn2).start()

            @pl.when(z < Z - 2)
            def _():
                z_copy(g, f, i, u_send, up2).start()

    def ff_y(g, zq, k, i):
        b = piece(g, wb[g], 2 * (2 * zq + y) + (x, ox)[k], i)
        return rcopy(b, b, y_send.at[g, zq, k, i], y_recv.at[g, zq, k, i], dy)

    def ff_y_own(g, k):
        for i in range(SUBS[g]):
            ff_y(g, z, k, i).start()

    def ff_y_wait(g, zq, k, i):
        b = piece(g, wb[g], 2 * (2 * zq + oy) + (x, ox)[k], i)
        rcopy(b, b, y_send.at[g, zq, k, i], y_recv.at[g, zq, k, i], dy).wait_recv()

    def ff_x_wait(g, q, i):
        b = piece(g, wb[g], 2 * q + ox, i)
        rcopy(b, b, x_send.at[g, q, i], x_recv.at[g, q, i], dx).wait_recv()

    def both_sides(g, d, act_on):
        for i in range(SUBS[g]):
            @pl.when(z >= d)
            def _():
                act_on(z - d, -1, i)

            @pl.when(z + d < Z)
            def _():
                act_on(z + d, 1, i)

    def ff_arrive(g, d):
        def act_on(zq, side, i):
            q = 2 * zq + y
            z_copy(g, q, i, u_send, up).wait_recv()
            if side < 0:
                @pl.when(z < Z - 2)
                def _():
                    z_copy(g, q, i, u_send, up2).start()
            else:
                @pl.when(z >= 2)
                def _():
                    z_copy(g, q, i, d_send, dn2).start()
            x_copy(g, q, i).start()
            ff_y(g, zq, 0, i).start()

        both_sides(g, d, act_on)

    def ff_relay(g, d):
        def act_on(zq, side, i):
            if (g, d) in VIA_X:
                ff_y_wait(g, zq, 0, i)
                x_copy(g, 2 * zq + oy, i).start()
            else:
                ff_x_wait(g, 2 * zq + y, i)
                ff_y(g, zq, 1, i).start()

        both_sides(g, d, act_on)

    def ff_done(g):
        for i in range(SUBS[g]):
            for k in range(2):
                ff_y_wait(g, z, k, i)
        for d in range(1, Z):
            def act_on(zq, side, i):
                if (g, d) in VIA_X:
                    ff_x_wait(g, 2 * zq + y, i)
                    ff_x_wait(g, 2 * zq + oy, i)
                else:
                    ff_y_wait(g, zq, 0, i)
                    ff_y_wait(g, zq, 1, i)

            both_sides(g, d, act_on)

    def ff_drain(g):
        for i in range(SUBS[g]):
            b = piece(g, wb[g], 2 * f + x, i)
            t = piece(g, theirs[g], 0, i)

            @pl.when(z > 0)
            def _():
                rcopy(t, b, t_send.at[g, 0, i], z_recv.at[g, f, i], dn).wait_send()

            @pl.when(z < Z - 1)
            def _():
                rcopy(t, b, t_send.at[g, 1, i], z_recv.at[g, f, i], up).wait_send()

            @pl.when(z >= 2)
            def _():
                z_copy(g, f, i, d_send, dn2).wait_send()

            @pl.when(z < Z - 2)
            def _():
                z_copy(g, f, i, u_send, up2).wait_send()

            for k in range(2):
                ff_y(g, z, k, i).wait_send()
        for d in range(1, Z):
            def act_on(zq, side, i):
                q = 2 * zq + y
                if side < 0:
                    @pl.when(z < Z - 2)
                    def _():
                        z_copy(g, q, i, u_send, up2).wait_send()
                else:
                    @pl.when(z >= 2)
                    def _():
                        z_copy(g, q, i, d_send, dn2).wait_send()
                x_copy(g, q, i).wait_send()
                ff_y(g, zq, 0, i).wait_send()
                if (g, d) in VIA_X:
                    x_copy(g, 2 * zq + oy, i).wait_send()
                else:
                    ff_y(g, zq, 1, i).wait_send()

            both_sides(g, d, act_on)

    crows = pl.ds(c * SH, SH)
    orows = pl.ds(oc * SH, SH)
    tok_z = rcopy(tokens.at[crows], tokv.at[a, crows], tok_sem.at[0], tok_sem.at[1], dz)
    there = tokv.at[oa, crows]
    tok_core = rcopy(there, there, tok_sem.at[2], tok_sem.at[3], dc)
    for k in range(2):
        round_rows(0, 0, 0, gate_w, H, k)
        round_rows(0, H, 1, up_w, H, k)
    ff_own(0)
    ff_y_own(0, 0)
    fetch_start(0, down_w, 2 * H)
    fetch_start(1, value_w, 2 * C)
    tok_z.start()
    for k in range(2):
        round_rows(1, 0, 0, down_w, H, k)
    fetch_start(0, glu_w, 2 * C)
    for k in range(2):
        round_rows(2, 0, 1, value_w, C, k)
    fetch_start(1, out_w, 2 * C)
    for k in range(2):
        round_rows(2, C, 0, glu_w, C, k)
    for k in range(2):
        round_rows(3, 0, 1, out_w, C, k)
    for j in range(1, F):
        rcopy(sc, scl.at[f], s_send.at[j], s_recv.at[f], {"fs": lax.rem(f + j, F)}).start()

    def norm(v, gains):
        return (v * lax.rsqrt(jnp.mean(v * v, axis=-1, keepdims=True) + EPSILON) * gains).astype(jnp.bfloat16)

    def norm_tokens(s):
        @pl.loop(0, S // ROWS)
        def _(i):
            r = pl.ds(i * ROWS, ROWS)
            xa[s, r, :] = norm(tokv[s, r, :].astype(jnp.float32), first_gain[...])

    def gate_up(src, s):
        @pl.loop(0, H // TILE)
        def _(j):
            lo = pl.multiple_of(j * TILE, TILE)
            rows = src[s]
            gw = wb0[:, :, pl.ds(lo, TILE)].reshape(D, TILE)
            uw = wb0[:, :, pl.ds(H + lo, TILE)].reshape(D, TILE)
            gv = jnp.dot(rows, gw, preferred_element_type=jnp.float32) * gate_scale[:, pl.ds(pl.multiple_of(a * H + lo, LANES), TILE)]
            uv = jnp.dot(rows, uw, preferred_element_type=jnp.float32) * up_scale[:, pl.ds(pl.multiple_of(a * H + lo, LANES), TILE)]
            hid[s, :, pl.ds(lo, TILE)] = (gv * jax.nn.sigmoid(gv) * uv).astype(jnp.bfloat16)

    def project(src, w, width, s, first=0, last=F):
        @pl.loop(first, last)
        def _(j):
            rows = w[pl.ds(2 * j, 2)].reshape(R, width)
            p = lax.dot_general(src[s], rows, NT, preferred_element_type=jnp.float32)
            part[s, :, pl.ds(pl.multiple_of(j * R, R), R)] = p.astype(jnp.bfloat16)

    SIDES = ((a, oa, dz), (y, oy, dy), (a, oa, dz))

    def rs_core(u, s):
        return rcopy(part.at[s, orows], rc.at[u, s], rc_send.at[u, s], rc_recv.at[u, s], dc)

    def rs_pair(u, k):
        r = pl.ds(k * CHUNK, CHUNK)
        return rcopy(ys.at[u, r], ry.at[u, r], ry_send.at[u, k], ry_recv.at[u, k], SIDES[u][2])

    def rs_push(u):
        ot = SIDES[u][1]
        rs_core(u, ot).wait_recv()
        for k in range(K):
            @pl.loop(0, CHUNK // ROWS)
            def _(i):
                r = pl.ds(k * CHUNK + i * ROWS, ROWS)
                p = part[ot, pl.ds(c * SH + k * CHUNK + i * ROWS, ROWS), :].astype(jnp.float32)
                ys[u, r, :] = (p + rc[u, ot, r, :].astype(jnp.float32)).astype(jnp.bfloat16)

            rs_pair(u, k).start()

    def rs_finish(u, base, factor, scale_row, gains, dst):
        me, slot = SIDES[u][0], SIDES[u + 1][0]
        rs_core(u, me).wait_recv()
        for k in range(K):
            rs_pair(u, k).wait_recv()

            @pl.loop(0, CHUNK // ROWS)
            def _(i):
                r = pl.ds(k * CHUNK + i * ROWS, ROWS)
                rr = pl.ds(c * SH + k * CHUNK + i * ROWS, ROWS)
                total = part[me, rr, :].astype(jnp.float32) + rc[u, me, r, :].astype(jnp.float32)
                total = total + ry[u, r, :].astype(jnp.float32)
                b = tokv[me, rr, :] if base is None else res[base, r, :]
                now = (b.astype(jnp.float32) + dsc[scale_row:scale_row + 1, :] * factor * total).astype(jnp.bfloat16)
                res[u, r, :] = now
                dst[slot, rr, :] = norm(now.astype(jnp.float32), gains[...])

            ag_copy(u, 1, k, dst).start()
            ag_copy(u, 0, k, dst).start()

    def ag_rows(k, side):
        return pl.ds(side * SH + k * CHUNK, CHUNK)

    def ag_copy(u, kind, k, buf):
        me, ot, partner = SIDES[u + 1]
        b = buf.at[ot if kind == 2 else me, ag_rows(k, c)]
        return rcopy(b, b, ag_send.at[u, kind, k], ag_recv.at[u, kind, k], partner if kind == 1 else dc)

    def ag_wait(u, kind, k, buf):
        me, ot, _ = SIDES[u + 1]
        b = buf.at[me if kind == 0 else ot, ag_rows(k, c if kind == 1 else oc)]
        rcopy(b, b, ag_send.at[u, kind, k], ag_recv.at[u, kind, k], dc).wait_recv()

    def ag_pass(u, buf, first, last):
        for k in range(first, last):
            ag_wait(u, 1, k, buf)
            ag_copy(u, 2, k, buf).start()

    def ag_own(u, buf):
        for k in range(K):
            ag_wait(u, 0, k, buf)

    def ag_other(u, buf):
        for k in range(K):
            ag_wait(u, 2, k, buf)

    def fc_copy(s, q):
        cols = pl.ds(q * DC, DC)
        return rcopy(part.at[s, orows, cols], rc.at[2, s, :, cols], fc_send.at[s, q], fc_recv.at[s, q], dc)

    def fy_copy(q):
        cols = pl.ds(q * DC, DC)
        return rcopy(ys.at[2, :, cols], ry.at[2, :, cols], fy_send.at[q], fy_recv.at[q], dz)

    def last_push(q):
        cols = pl.ds(q * DC, DC)
        fc_copy(oa, q).wait_recv()

        @pl.loop(0, SH // ROWS)
        def _(i):
            r = pl.ds(i * ROWS, ROWS)
            p = part[oa, pl.ds(c * SH + i * ROWS, ROWS), cols].astype(jnp.float32)
            ys[2, r, cols] = (p + rc[2, oa, r, cols].astype(jnp.float32)).astype(jnp.bfloat16)

        fy_copy(q).start()

    def out_copies(q):
        cols = pl.ds(q * DC, DC)
        src, dst = res.at[2, :, cols], out.at[crows, cols]
        return pltpu.make_async_copy(src, dst, out_sem.at[q]), rcopy(src, dst, oc_send.at[q], oc_recv.at[q], dc)

    def last_finish(q):
        cols = pl.ds(q * DC, DC)
        fc_copy(a, q).wait_recv()
        fy_copy(q).wait_recv()

        @pl.loop(0, SH // ROWS)
        def _(i):
            r = pl.ds(i * ROWS, ROWS)
            total = part[a, pl.ds(c * SH + i * ROWS, ROWS), cols].astype(jnp.float32) + rc[2, a, r, cols].astype(jnp.float32)
            total = total + ry[2, r, cols].astype(jnp.float32)
            res[2, r, cols] = (res[1, r, cols].astype(jnp.float32) + 0.5 * dsc[0:1, cols] * total).astype(jnp.bfloat16)

        for cp in out_copies(q):
            cp.start()

    def value_glu(s):
        @pl.loop(0, C // TILE)
        def _(j):
            lo = pl.multiple_of(j * TILE, TILE)
            rows = xb[s]
            vw = wb2[:, :, pl.ds(lo, TILE)].reshape(D, TILE)
            gw = wb2[:, :, pl.ds(C + lo, TILE)].reshape(D, TILE)
            vv = jnp.dot(rows, vw, preferred_element_type=jnp.float32) * value_scale[:, pl.ds(pl.multiple_of(y * C + lo, LANES), TILE)]
            gv = jnp.dot(rows, gw, preferred_element_type=jnp.float32) * glu_scale[:, pl.ds(pl.multiple_of(y * C + lo, LANES), TILE)]
            g = (vv * jax.nn.sigmoid(gv)).astype(jnp.bfloat16)
            gp[s, pl.ds(PAD, S), pl.ds(lo, TILE)] = g.astype(jnp.float32)

    def convolve(s):
        @pl.loop(0, C // LANES)
        def _(j):
            cols = pl.ds(pl.multiple_of(j * LANES, LANES), LANES)
            near = pl.ds(pl.multiple_of(y * C + j * LANES, LANES), LANES)
            gp[s, pl.ds(0, PAD), cols] = jnp.zeros((PAD, LANES), jnp.float32)
            total = jnp.zeros((S, LANES), jnp.float32)
            for k in range(KW):
                total = total + conv_k[k:k + 1, near] * gp[s, pl.ds(PAD - (KW - 1) + k, S), cols]
            mixed[s, :, cols] = total

        m = mixed[s]
        low = lax.broadcasted_iota(jnp.int32, (8, C), 0) < 4
        one, nil = jnp.ones((8, C), jnp.float32), jnp.zeros((8, C), jnp.float32)
        hi = lax.Precision.HIGHEST
        sums = lax.dot_general(jnp.where(low, one, nil), m, NT, precision=hi, preferred_element_type=jnp.float32)
        squares = lax.dot_general(jnp.where(low, nil, one), m * m, NT, precision=hi, preferred_element_type=jnp.float32)
        st[0, s] = sums + squares

    def st_copies():
        return [rcopy(st.at[0], st.at[k + 1], st_send.at[k], st_recv.at[k], dev) for k, dev in enumerate((dc, dy, dyc))]

    def activate(s):
        total = st[0, s] + st[1, s] + st[2, s] + st[3, s]
        total = total / D
        mean, square = total[0:1], total[4:5]
        rstd = lax.rsqrt(square - mean * mean + EPSILON)
        row = lax.broadcasted_iota(jnp.int32, (8, S), 0)
        both = jnp.where(row == 0, jnp.broadcast_to(mean, (8, S)), jnp.where(row == 1, jnp.broadcast_to(rstd, (8, S)), 0.0))
        pick = lax.broadcasted_iota(jnp.int32, (8, LANES), 0)
        hi = lax.Precision.HIGHEST
        mcol = lax.dot_general(both, jnp.where(pick == 0, 1.0, 0.0), TN, precision=hi, preferred_element_type=jnp.float32)
        rcol = lax.dot_general(both, jnp.where(pick == 1, 1.0, 0.0), TN, precision=hi, preferred_element_type=jnp.float32)
        for j in range(C // LANES):
            cols = slice(j * LANES, (j + 1) * LANES)
            v = (mixed[s, :, cols] - mcol) * rcol * norm_gain[:, pl.ds(pl.multiple_of(y * C + j * LANES, LANES), LANES)]
            act[s, :, cols] = (v * jax.nn.sigmoid(v)).astype(jnp.bfloat16)

    tok_local.wait()
    norm_tokens(a)
    ff_arrive(0, 1)
    ff_y_own(0, 1)
    ff_own(1)
    ff_arrive(0, 2)
    ff_relay(0, 1)
    for d in range(3, Z):
        ff_arrive(0, d)
    y_start(2, 0)
    y_start(3, 0)
    ff_y_own(1, 0)
    ff_arrive(1, 1)
    ff_relay(0, 2)
    rcopy(there, there, tok_sem.at[0], tok_sem.at[1], dz).wait_recv()
    tok_core.start()
    send_rows(2, f, False)
    send_rows(3, f, False)
    send_rows(2, fp, True)
    send_rows(3, fp, True)
    ff_arrive(1, 2)
    for d in range(3, Z):
        ff_arrive(1, d)
    ff_y_own(1, 1)
    for d in range(3, Z):
        ff_relay(0, d)
    b = tokv.at[oa, orows]
    rcopy(b, b, tok_sem.at[2], tok_sem.at[3], dc).wait_recv()
    norm_tokens(oa)
    forward(2, 1)
    forward(2, 2)
    ff_relay(1, 1)
    ff_relay(1, 2)
    for d in range(3, Z):
        forward(2, d)
    for d in range(3, Z):
        ff_relay(1, d)
    forward(3, 1)
    forward(3, 2)
    ff_done(0)
    gate_up(xa, oa)
    for d in range(3, Z):
        forward(3, d)
    gate_up(xa, a)
    ff_done(1)
    y_start(2, 1)
    y_start(3, 1)
    project(hid, wb1, H, oa)
    rs_core(0, oa).start()
    project(hid, wb1, H, a)
    rs_core(0, a).start()
    rs_push(0)
    for j in range(1, F):
        b = scl.at[lax.rem(f + j, F)]
        rcopy(b, b, s_send.at[j], s_recv.at[lax.rem(f + j, F)], dy).wait_recv()
    scl[f] = sc[...]
    for j in range(F):
        dsc[:, j * R:(j + 1) * R] = scl[j]
    rs_finish(0, None, 0.5, 0, conv_gain, xb)
    ag_pass(0, xb, 0, K)
    ag_own(0, xb)
    group_done(2)
    value_glu(y)
    convolve(y)
    ag_other(0, xb)
    value_glu(oy)
    convolve(oy)
    for cp in st_copies():
        cp.start()
    for s in range(2):
        rs_core(0, s).wait_send()
    for cp in st_copies():
        cp.wait()
    group_done(3)
    activate(oy)
    project(act, wb3, C, oy)
    rs_core(1, oy).start()
    activate(y)
    project(act, wb3, C, y)
    rs_core(1, y).start()
    rs_push(1)
    for g in (0, 1):
        ff_drain(g)
    for g in (2, 3):
        drain(g)
    rs_finish(1, 0, 1.0, 1, second_gain, xc)
    ag_own(1, xc)
    gate_up(xc, a)
    for s in range(2):
        rs_core(1, s).wait_send()
    ag_pass(1, xc, 0, K)
    ag_other(1, xc)
    gate_up(xc, oa)
    step = F // COLS
    for q in range(COLS):
        project(hid, wb1, H, oa, q * step, (q + 1) * step)
        fc_copy(oa, q).start()
        if q:
            last_push(q - 1)
    for q in range(COLS):
        project(hid, wb1, H, a, q * step, (q + 1) * step)
        fc_copy(a, q).start()
        if q == 0:
            last_push(COLS - 1)
    tok_z.wait_send()
    tok_core.wait_send()
    for j in range(1, F):
        rcopy(sc, scl.at[f], s_send.at[j], s_recv.at[f], dy).wait_send()
    for u, buf in enumerate((xb, xc)):
        for k in range(K):
            rs_pair(u, k).wait_send()
            for kind in range(3):
                ag_copy(u, kind, k, buf).wait_send()
    for q in range(COLS):
        last_finish(q)
    for q in range(COLS):
        for s in range(2):
            fc_copy(s, q).wait_send()
        fy_copy(q).wait_send()
        near, far = out_copies(q)
        near.wait()
        far.wait_send()
        b = out.at[orows, pl.ds(q * DC, DC)]
        rcopy(b, b, oc_send.at[q], oc_recv.at[q], dc).wait_recv()


def local_fused(tokens, gate_weight, up_weight, down_weight, value_weight, glu_weight, out_weight, gate_scale, up_scale,
                down_scale, value_scale, glu_scale, out_scale, conv_kernel, norm_gain, first_gain, conv_gain, second_gain):
    F = lax.axis_size("fs")
    S, D = tokens.shape
    R, H = gate_weight.shape[0], gate_weight.shape[1] // 2
    C = value_weight.shape[1] // 2
    KW = conv_kernel.shape[0]
    RX = R // 2
    SH = S // 2
    vectors = (down_scale, out_scale, first_gain, conv_gain, second_gain, gate_scale, up_scale, value_scale, glu_scale, norm_gain)
    rows = [v.reshape(1, -1) for v in vectors]
    widths = (2 * H, H, 2 * C, C)
    G, K, NS = len(widths), SH // CHUNK, max(SUBS)
    bf, f32 = jnp.bfloat16, jnp.float32
    dma = pltpu.SemaphoreType.DMA
    anyspace = pl.BlockSpec(memory_space=pl.ANY)
    vmem = pl.BlockSpec(memory_space=pltpu.VMEM)
    pad = -(-(KW - 1) // 8) * 8
    return pl.pallas_call(
        functools.partial(fused_kernel, (S, D, H, C, KW, F, RX)),
        out_shape=jax.ShapeDtypeStruct((S, D), bf),
        in_specs=[anyspace] * 7 + [vmem] * 11,
        out_specs=anyspace,
        scratch_shapes=[pltpu.VMEM((2 * F, RX, w), bf) for w in widths]
        + [pltpu.VMEM((1 if g < 2 else 2, RX, w), bf) for g, w in enumerate(widths)]
        + [pltpu.VMEM((2, R, 2 * H), f32)]
        + [pltpu.VMEM((2, S, D), bf)] * 4
        + [pltpu.VMEM((2, S, H), bf), pltpu.VMEM((2, S, D), bf)]
        + [pltpu.VMEM((3, 2, SH, D), bf), pltpu.VMEM((3, SH, D), bf), pltpu.VMEM((3, SH, D), bf), pltpu.VMEM((3, SH, D), bf)]
        + [pltpu.VMEM((2, S + pad, C), f32), pltpu.VMEM((2, S, C), f32), pltpu.VMEM((2, S, C), bf)]
        + [pltpu.VMEM((4, 2, 8, S), f32), pltpu.VMEM((8, R), f32), pltpu.VMEM((F, 8, R), f32), pltpu.VMEM((8, D), f32)]
        + [dma((2, 2)), dma((G, F // 2, 2, NS)), dma((G, F // 2, 2, NS))] + [dma((G, F, NS))] * 2 + [dma((2, 2, NS))] + [dma((G, F, NS))] * 3
        + [dma((4,)), dma((F,)), dma((F,))]
        + [dma((3, 2)), dma((3, 2)), dma((2, K)), dma((2, K)), dma((2, 3, K)), dma((2, 3, K))]
        + [dma((2, COLS)), dma((2, COLS)), dma((COLS,)), dma((COLS,))]
        + [dma((3,)), dma((3,)), dma((COLS,)), dma((COLS,)), dma((COLS,))],
        compiler_params=pltpu.CompilerParams(
            collective_id=0, has_side_effects=True, vmem_limit_bytes=64 * 1024 * 1024 - 65536
        ),
    )(tokens, gate_weight, up_weight, down_weight, value_weight, glu_weight, out_weight, *rows, conv_kernel)


def rms_rows(rows, gains):
    values = rows.astype(jnp.float32)
    scaled = values * lax.rsqrt(jnp.mean(values * values, axis=-1, keepdims=True) + EPSILON)
    return (scaled * gains).astype(jnp.bfloat16)


def gated_hidden(normed, gate_full, up_full, gate_scale, up_scale):
    gate_part = jnp.dot(normed, gate_full, preferred_element_type=jnp.float32) * gate_scale
    upward = jnp.dot(normed, up_full, preferred_element_type=jnp.float32) * up_scale
    return (jax.nn.silu(gate_part) * upward).astype(jnp.bfloat16)


def causal_depthwise(inputs, kernel):
    taps = kernel.shape[0]
    length = inputs.shape[0]
    padded = jnp.concatenate(
        [jnp.zeros((taps - 1, inputs.shape[1]), jnp.float32), inputs.astype(jnp.float32)], axis=0
    )
    total = jnp.zeros((length, inputs.shape[1]), jnp.float32)
    for offset in range(taps):
        total = total + kernel[offset] * padded[offset : offset + length]
    return total


def swap(values, axis):
    return lax.ppermute(values, axis, [(0, 1), (1, 0)])


def gather_rows(rows, axis):
    if lax.axis_size(axis) != 2:
        return lax.all_gather(rows, axis, axis=0, tiled=True)
    other = swap(rows, axis)
    first = lax.axis_index(axis) == 0
    return jnp.concatenate([jnp.where(first, rows, other), jnp.where(first, other, rows)], axis=0)


def scatter_rows(partial, axis):
    members = lax.axis_size(axis)
    if members != 2:
        return lax.psum_scatter(partial, axis, scatter_dimension=0, tiled=True).astype(jnp.float32)
    own_rows = partial.shape[0] // members
    place = lax.axis_index(axis)
    mine = lax.dynamic_slice_in_dim(partial, place * own_rows, own_rows, 0)
    theirs = lax.dynamic_slice_in_dim(partial, (1 - place) * own_rows, own_rows, 0)
    return mine.astype(jnp.float32) + swap(theirs, axis).astype(jnp.float32)


def pull(rows, step):
    n = lax.axis_size("rep")
    return lax.ppermute(rows, "rep", [(s, (s - step) % n) for s in range(n)])


def push(rows, step):
    n = lax.axis_size("rep")
    return lax.ppermute(rows, "rep", [(s, (s + step) % n) for s in range(n)])


def streams_of(own):
    n = lax.axis_size("rep")
    parts = [own] + [pull(own, step) for step in range(1, n)]
    return [gather_rows(part, "tp") for part in parts]


def owned_sum(actives, weight_rows):
    n = lax.axis_size("rep")
    total = None
    for step in list(range(1, n)) + [0]:
        partial = lax.dot_general(
            actives[step], weight_rows, (((1,), (1,)), ((), ())), preferred_element_type=jnp.float32
        ).astype(jnp.bfloat16)
        part = scatter_rows(partial, "tp")
        if step:
            part = push(part.astype(jnp.bfloat16), step).astype(jnp.float32)
        total = part if total is None else total + part
    return total


def local_plain(
    tokens,
    gate_weight,
    up_weight,
    down_weight,
    value_weight,
    glu_weight,
    out_weight,
    gate_scale,
    up_scale,
    down_scale,
    value_scale,
    glu_scale,
    out_scale,
    conv_kernel,
    norm_gain,
    first_gain,
    conv_gain,
    second_gain,
):
    reps = lax.axis_size("rep")
    rep = lax.axis_index("rep")

    def part(array, dim):
        width = array.shape[dim] // reps
        return lax.dynamic_slice_in_dim(array, rep * width, width, dim)

    scales = lax.all_gather(jnp.stack([down_scale, out_scale]), "fs", axis=1, tiled=True)
    down_rows, out_rows = scales[0], scales[1]

    def full(weight):
        return lax.all_gather(part(weight, 1).astype(jnp.bfloat16), "fs", axis=0, tiled=True)

    gate_full, up_full, down_full, value_full, glu_full, out_full = (
        full(gate_weight),
        full(up_weight),
        full(down_weight),
        full(value_weight),
        full(glu_weight),
        full(out_weight),
    )
    gate_scale, up_scale, value_scale, glu_scale, norm_gain = (
        part(gate_scale, 0),
        part(up_scale, 0),
        part(value_scale, 0),
        part(glu_scale, 0),
        part(norm_gain, 0),
    )
    conv_kernel = part(conv_kernel, 1)
    members = lax.axis_size("tp")
    own_rows = tokens.shape[0] // members
    own_tokens = lax.dynamic_slice_in_dim(tokens, lax.axis_index("tp") * own_rows, own_rows, 0)

    normed = rms_rows(tokens, first_gain)
    own_normed = rms_rows(own_tokens, first_gain)
    rows = [normed] + [gather_rows(pull(own_normed, step), "tp") for step in range(1, reps)]
    hidden = [gated_hidden(r, gate_full, up_full, gate_scale, up_scale) for r in rows]
    after_first = (
        own_tokens.astype(jnp.float32) + 0.5 * down_rows * owned_sum(hidden, down_full)
    ).astype(jnp.bfloat16)
    mixes, sums = [], []
    for rows in streams_of(rms_rows(after_first, conv_gain)):
        value_part = jnp.dot(rows, value_full, preferred_element_type=jnp.float32) * value_scale
        gate_part = jnp.dot(rows, glu_full, preferred_element_type=jnp.float32) * glu_scale
        glu_in = (value_part * jax.nn.sigmoid(gate_part)).astype(jnp.bfloat16)
        mixed = causal_depthwise(glu_in, conv_kernel)
        mixes.append(mixed)
        sums.append(jnp.stack([jnp.sum(mixed, axis=1), jnp.sum(mixed * mixed, axis=1)]))
    totals = lax.psum(jnp.roll(jnp.stack(sums), rep, axis=0), ("rep", "tp"))
    totals = jnp.roll(totals, -rep, axis=0) / (norm_gain.shape[0] * reps * lax.axis_size("tp"))
    actives = []
    for step, mixed in enumerate(mixes):
        mean_rows = totals[step, 0][:, None]
        square_rows = totals[step, 1][:, None]
        normalized = (
            (mixed - mean_rows) * lax.rsqrt(square_rows - mean_rows * mean_rows + EPSILON) * norm_gain
        )
        actives.append(jax.nn.silu(normalized).astype(jnp.bfloat16))
    after_conv = (after_first.astype(jnp.float32) + out_rows * owned_sum(actives, out_full)).astype(
        jnp.bfloat16
    )
    hidden = [
        gated_hidden(r, gate_full, up_full, gate_scale, up_scale)
        for r in streams_of(rms_rows(after_conv, second_gain))
    ]
    after_second = (
        after_conv.astype(jnp.float32) + 0.5 * down_rows * owned_sum(hidden, down_full)
    ).astype(jnp.bfloat16)
    return gather_rows(after_second, "tp")


def fits(mesh):
    return mesh.shape["rep"] == 2 and mesh.shape["tp"] == 2 and mesh.shape["fs"] % 4 == 0


def solution(mesh):
    columns, rows = P("fs", "tp"), P(("rep", "fs"), None)
    placed = (rows,) + (columns,) * 6 + (P("tp"), P("tp"), P("fs"), P("tp"), P("tp"), P("fs"), P(None, "tp"), P("tp"), P(), P(), P())
    local = local_fused if fits(mesh) else local_plain
    return jax.shard_map(local, mesh=mesh, in_specs=placed, out_specs=rows, check_vma=False)
```

```python
import functools

import jax
import jax.numpy as jnp
from jax import lax
from jax.experimental import pallas as pl
from jax.experimental.pallas import tpu as pltpu
from jax.sharding import PartitionSpec as P

MESH = pl.DeviceIdType.MESH
EPSILON = 1e-06
LANES = 128
TILE = 256
ROWS = 16
CHUNK = 32
SUBS = (2, 1, 1, 1)
VIA_X = ((0, 1), (0, 2), (0, 3))
COLS = 4
NT = (((1,), (1,)), ((), ()))
TN = (((0,), (0,)), ((), ()))


def fused_kernel(dims, *refs):
    S, D, H, C, KW, F, RX = dims
    Z = F // 2
    SH = S // 2
    R = 2 * RX
    PAD = -(-(KW - 1) // 8) * 8
    K, DC = SH // CHUNK, D // COLS
    (tokens, gate_w, up_w, down_w, value_w, glu_w, out_w, down_scale, out_scale, first_gain, conv_gain, second_gain,
     gate_scale, up_scale, value_scale, glu_scale, norm_gain, conv_k, out, *scratch) = refs
    (wb0, wb1, wb2, wb3, t0, t1, t2, t3, sg, tokv, xa, xb, xc, hid, part, rc, ry, ys, res, gp, mixed, act, st, sc, scl, dsc,
     f_sem, y_send, y_recv, u_send, d_send, t_send, z_recv, x_send, x_recv, tok_sem, s_send, s_recv,
     rc_send, rc_recv, ry_send, ry_recv, ag_send, ag_recv, fc_send, fc_recv, fy_send, fy_recv,
     st_send, st_recv, out_sem, oc_send, oc_recv) = scratch
    theirs, wb = (t0, t1, t2, t3), (wb0, wb1, wb2, wb3)
    G = len(wb)

    x = lax.axis_index("rep")
    f = lax.axis_index("fs")
    c = lax.axis_index("tp")
    y = lax.rem(f, 2)
    z = lax.div(f, 2)
    fp = f + 1 - 2 * y
    ox, oy, oc = 1 - x, 1 - y, 1 - c
    a = lax.rem(z, 2)
    oa = 1 - a
    dx, dc, dy, dyc = {"rep": ox}, {"tp": oc}, {"fs": fp}, {"fs": fp, "tp": oc}
    dz = {"fs": f + 2 - 4 * a}
    up, dn = {"fs": f + 2}, {"fs": f - 2}
    up2, dn2 = {"fs": f + 4}, {"fs": f - 4}

    def rcopy(src, dst, ssem, rsem, dev):
        return pltpu.make_async_remote_copy(
            src_ref=src, dst_ref=dst, send_sem=ssem, recv_sem=rsem, device_id=dev, device_id_type=MESH
        )

    def fetch(slot, ref, width, h, k):
        rows = pl.ds(h * RX, RX)
        return pltpu.make_async_copy(ref.at[rows], sg.at[slot, rows, pl.ds(0, width)], f_sem.at[slot, k])

    def fetch_start(slot, ref, width):
        for k, h in enumerate((x, ox)):
            fetch(slot, ref, width, h, k).start()

    def round_rows(g, off, slot, ref, width, k):
        h = (x, ox)[k]
        side = a if g < 2 else y
        fetch(slot, ref, 2 * width, h, k).wait()

        @pl.loop(0, RX // ROWS)
        def _(i):
            rows = pl.ds(h * RX + i * ROWS, ROWS)
            r = pl.ds(i * ROWS, ROWS)
            near = sg[slot, rows, pl.ds(pl.multiple_of(side * width, LANES), width)]
            wb[g][2 * f + h, r, off:off + width] = near.astype(jnp.bfloat16)
            if g >= 2 or k == 0:
                far = sg[slot, rows, pl.ds(pl.multiple_of((1 - side) * width, LANES), width)]
                theirs[g][h if g >= 2 else 0, r, off:off + width] = far.astype(jnp.bfloat16)

    fetch_start(0, gate_w, 2 * H)
    fetch_start(1, up_w, 2 * H)
    tok_local = pltpu.make_async_copy(tokens, tokv.at[a], out_sem.at[0])
    tok_local.start()
    sc[...] = jnp.zeros_like(sc)
    sc[0:1, :] = down_scale[...]
    sc[1:2, :] = out_scale[...]

    barrier = pltpu.get_barrier_semaphore()
    for j in range(1, F):
        pl.semaphore_signal(barrier, inc=1, device_id={"fs": lax.rem(f + j, F)}, device_id_type=MESH)
    for dev in (dx, dc, dyc):
        pl.semaphore_signal(barrier, inc=1, device_id=dev, device_id_type=MESH)
    pl.semaphore_wait(barrier, F + 2)

    def piece(g, ref, lead, i):
        n = RX // SUBS[g]
        return ref.at[lead, pl.ds(i * n, n)]

    def y_copy(g, h, k, i):
        return rcopy(piece(g, theirs[g], h, i), piece(g, wb[g], 2 * f + h, i), y_send.at[g, 0, k, i], y_recv.at[g, 0, k, i], dy)

    def y_start(g, k):
        for i in range(SUBS[g]):
            y_copy(g, (x, ox)[k], k, i).start()

    def y_wait(g, h, k, i):
        b = piece(g, wb[g], 2 * fp + h, i)
        rcopy(b, b, y_send.at[g, 0, k, i], y_recv.at[g, 0, k, i], dy).wait_recv()

    def z_copy(g, q, i, sems, dev):
        b = piece(g, wb[g], 2 * q + x, i)
        return rcopy(b, b, sems.at[g, q, i], z_recv.at[g, q, i], dev)

    def x_copy(g, q, i):
        b = piece(g, wb[g], 2 * q + x, i)
        return rcopy(b, b, x_send.at[g, q, i], x_recv.at[g, q, i], dx)

    def send_rows(g, q, wait):
        for i in range(SUBS[g]):
            if wait:
                y_wait(g, x, 0, i)

            @pl.when(z < Z - 1)
            def _():
                z_copy(g, q, i, u_send, up).start()

            @pl.when(z > 0)
            def _():
                z_copy(g, q, i, d_send, dn).start()

    def forward(g, d):
        for k in range(2):
            yy = y if k == 0 else oy
            for i in range(SUBS[g]):
                @pl.when(z >= d)
                def _():
                    q = 2 * (z - d) + yy
                    z_copy(g, q, i, u_send, up).wait_recv()

                    @pl.when(z < Z - 1)
                    def _():
                        z_copy(g, q, i, u_send, up).start()

                    x_copy(g, q, i).start()

                @pl.when(z + d < Z)
                def _():
                    q = 2 * (z + d) + yy
                    z_copy(g, q, i, d_send, dn).wait_recv()

                    @pl.when(z > 0)
                    def _():
                        z_copy(g, q, i, d_send, dn).start()

                    x_copy(g, q, i).start()

    def group_done(g):
        for i in range(SUBS[g]):
            y_wait(g, ox, 1, i)

        @pl.loop(0, F)
        def _(q):
            @pl.when(lax.div(q, 2) != z)
            def _():
                for i in range(SUBS[g]):
                    b = piece(g, wb[g], 2 * q + ox, i)
                    rcopy(b, b, x_send.at[g, q, i], x_recv.at[g, q, i], dx).wait_recv()

    def drain(g):
        for k, h in enumerate((x, ox)):
            for i in range(SUBS[g]):
                y_copy(g, h, k, i).wait_send()

        @pl.loop(0, F)
        def _(q):
            zq = lax.div(q, 2)

            @pl.when((z < Z - 1) & (zq <= z))
            def _():
                for i in range(SUBS[g]):
                    z_copy(g, q, i, u_send, up).wait_send()

            @pl.when((z > 0) & (zq >= z))
            def _():
                for i in range(SUBS[g]):
                    z_copy(g, q, i, d_send, dn).wait_send()

            @pl.when(zq != z)
            def _():
                for i in range(SUBS[g]):
                    x_copy(g, q, i).wait_send()

    def ff_own(g):
        for i in range(SUBS[g]):
            b = piece(g, wb[g], 2 * f + x, i)
            t = piece(g, theirs[g], 0, i)

            @pl.when(z > 0)
            def _():
                rcopy(t, b, t_send.at[g, 0, i], z_recv.at[g, f, i], dn).start()

            @pl.when(z < Z - 1)
            def _():
                rcopy(t, b, t_send.at[g, 1, i], z_recv.at[g, f, i], up).start()

            @pl.when(z >= 2)
            def _():
                z_copy(g, f, i, d_send, dn2).start()

            @pl.when(z < Z - 2)
            def _():
                z_copy(g, f, i, u_send, up2).start()

    def ff_y(g, zq, k, i):
        b = piece(g, wb[g], 2 * (2 * zq + y) + (x, ox)[k], i)
        return rcopy(b, b, y_send.at[g, zq, k, i], y_recv.at[g, zq, k, i], dy)

    def ff_y_own(g, k):
        for i in range(SUBS[g]):
            ff_y(g, z, k, i).start()

    def ff_y_wait(g, zq, k, i):
        b = piece(g, wb[g], 2 * (2 * zq + oy) + (x, ox)[k], i)
        rcopy(b, b, y_send.at[g, zq, k, i], y_recv.at[g, zq, k, i], dy).wait_recv()

    def ff_x_wait(g, q, i):
        b = piece(g, wb[g], 2 * q + ox, i)
        rcopy(b, b, x_send.at[g, q, i], x_recv.at[g, q, i], dx).wait_recv()

    def both_sides(g, d, act_on):
        for i in range(SUBS[g]):
            @pl.when(z >= d)
            def _():
                act_on(z - d, -1, i)

            @pl.when(z + d < Z)
            def _():
                act_on(z + d, 1, i)

    def ff_arrive(g, d):
        def act_on(zq, side, i):
            q = 2 * zq + y
            z_copy(g, q, i, u_send, up).wait_recv()
            if side < 0:
                @pl.when(z < Z - 2)
                def _():
                    z_copy(g, q, i, u_send, up2).start()
            else:
                @pl.when(z >= 2)
                def _():
                    z_copy(g, q, i, d_send, dn2).start()
            x_copy(g, q, i).start()
            ff_y(g, zq, 0, i).start()

        both_sides(g, d, act_on)

    def ff_relay(g, d):
        def act_on(zq, side, i):
            if (g, d) in VIA_X:
                ff_y_wait(g, zq, 0, i)
                x_copy(g, 2 * zq + oy, i).start()
            else:
                ff_x_wait(g, 2 * zq + y, i)
                ff_y(g, zq, 1, i).start()

        both_sides(g, d, act_on)

    def ff_done(g):
        for i in range(SUBS[g]):
            for k in range(2):
                ff_y_wait(g, z, k, i)
        for d in range(1, Z):
            def act_on(zq, side, i):
                if (g, d) in VIA_X:
                    ff_x_wait(g, 2 * zq + y, i)
                    ff_x_wait(g, 2 * zq + oy, i)
                else:
                    ff_y_wait(g, zq, 0, i)
                    ff_y_wait(g, zq, 1, i)

            both_sides(g, d, act_on)

    def ff_drain(g):
        for i in range(SUBS[g]):
            b = piece(g, wb[g], 2 * f + x, i)
            t = piece(g, theirs[g], 0, i)

            @pl.when(z > 0)
            def _():
                rcopy(t, b, t_send.at[g, 0, i], z_recv.at[g, f, i], dn).wait_send()

            @pl.when(z < Z - 1)
            def _():
                rcopy(t, b, t_send.at[g, 1, i], z_recv.at[g, f, i], up).wait_send()

            @pl.when(z >= 2)
            def _():
                z_copy(g, f, i, d_send, dn2).wait_send()

            @pl.when(z < Z - 2)
            def _():
                z_copy(g, f, i, u_send, up2).wait_send()

            for k in range(2):
                ff_y(g, z, k, i).wait_send()
        for d in range(1, Z):
            def act_on(zq, side, i):
                q = 2 * zq + y
                if side < 0:
                    @pl.when(z < Z - 2)
                    def _():
                        z_copy(g, q, i, u_send, up2).wait_send()
                else:
                    @pl.when(z >= 2)
                    def _():
                        z_copy(g, q, i, d_send, dn2).wait_send()
                x_copy(g, q, i).wait_send()
                ff_y(g, zq, 0, i).wait_send()
                if (g, d) in VIA_X:
                    x_copy(g, 2 * zq + oy, i).wait_send()
                else:
                    ff_y(g, zq, 1, i).wait_send()

            both_sides(g, d, act_on)

    crows = pl.ds(c * SH, SH)
    orows = pl.ds(oc * SH, SH)
    tok_z = rcopy(tokens.at[crows], tokv.at[a, crows], tok_sem.at[0], tok_sem.at[1], dz)
    there = tokv.at[oa, crows]
    tok_core = rcopy(there, there, tok_sem.at[2], tok_sem.at[3], dc)
    for k in range(2):
        round_rows(0, 0, 0, gate_w, H, k)
        round_rows(0, H, 1, up_w, H, k)
    ff_own(0)
    ff_y_own(0, 0)
    fetch_start(0, down_w, 2 * H)
    fetch_start(1, value_w, 2 * C)
    tok_z.start()
    for k in range(2):
        round_rows(1, 0, 0, down_w, H, k)
    fetch_start(0, glu_w, 2 * C)
    for k in range(2):
        round_rows(2, 0, 1, value_w, C, k)
    fetch_start(1, out_w, 2 * C)
    for k in range(2):
        round_rows(2, C, 0, glu_w, C, k)
    for k in range(2):
        round_rows(3, 0, 1, out_w, C, k)
    for j in range(1, F):
        rcopy(sc, scl.at[f], s_send.at[j], s_recv.at[f], {"fs": lax.rem(f + j, F)}).start()

    def norm(v, gains):
        return (v * lax.rsqrt(jnp.mean(v * v, axis=-1, keepdims=True) + EPSILON) * gains).astype(jnp.bfloat16)

    def norm_tokens(s):
        @pl.loop(0, S // ROWS)
        def _(i):
            r = pl.ds(i * ROWS, ROWS)
            xa[s, r, :] = norm(tokv[s, r, :].astype(jnp.float32), first_gain[...])

    def wide(ref, j):
        first, n = a * (H // LANES) + j * (TILE // LANES), TILE // LANES
        return jnp.concatenate([ref[pl.ds(first + t, 1), :] for t in range(n)], axis=1)

    def gate_up(src, s):
        @pl.loop(0, H // TILE)
        def _(j):
            lo = pl.multiple_of(j * TILE, TILE)
            rows = src[s]
            gw = wb0[:, :, pl.ds(lo, TILE)].reshape(D, TILE)
            uw = wb0[:, :, pl.ds(H + lo, TILE)].reshape(D, TILE)
            gv = jnp.dot(rows, gw, preferred_element_type=jnp.float32) * wide(gate_scale, j)
            uv = jnp.dot(rows, uw, preferred_element_type=jnp.float32) * wide(up_scale, j)
            hid[s, :, pl.ds(lo, TILE)] = (gv * jax.nn.sigmoid(gv) * uv).astype(jnp.bfloat16)

    def project(src, w, width, s, first=0, last=F):
        @pl.loop(first, last)
        def _(j):
            rows = w[pl.ds(2 * j, 2)].reshape(R, width)
            p = lax.dot_general(src[s], rows, NT, preferred_element_type=jnp.float32)
            part[s, :, pl.ds(pl.multiple_of(j * R, R), R)] = p.astype(jnp.bfloat16)

    SIDES = ((a, oa, dz), (y, oy, dy), (a, oa, dz))

    def rs_core(u, s):
        return rcopy(part.at[s, orows], rc.at[u, s], rc_send.at[u, s], rc_recv.at[u, s], dc)

    def rs_pair(u, k):
        r = pl.ds(k * CHUNK, CHUNK)
        return rcopy(ys.at[u, r], ry.at[u, r], ry_send.at[u, k], ry_recv.at[u, k], SIDES[u][2])

    def rs_push(u):
        ot = SIDES[u][1]
        rs_core(u, ot).wait_recv()
        for k in range(K):
            @pl.loop(0, CHUNK // ROWS)
            def _(i):
                r = pl.ds(k * CHUNK + i * ROWS, ROWS)
                p = part[ot, pl.ds(c * SH + k * CHUNK + i * ROWS, ROWS), :].astype(jnp.float32)
                ys[u, r, :] = (p + rc[u, ot, r, :].astype(jnp.float32)).astype(jnp.bfloat16)

            rs_pair(u, k).start()

    def rs_finish(u, base, factor, scale_row, gains, dst):
        me, slot = SIDES[u][0], SIDES[u + 1][0]
        rs_core(u, me).wait_recv()
        for k in range(K):
            rs_pair(u, k).wait_recv()

            @pl.loop(0, CHUNK // ROWS)
            def _(i):
                r = pl.ds(k * CHUNK + i * ROWS, ROWS)
                rr = pl.ds(c * SH + k * CHUNK + i * ROWS, ROWS)
                total = part[me, rr, :].astype(jnp.float32) + rc[u, me, r, :].astype(jnp.float32)
                total = total + ry[u, r, :].astype(jnp.float32)
                b = tokv[me, rr, :] if base is None else res[base, r, :]
                now = (b.astype(jnp.float32) + dsc[scale_row:scale_row + 1, :] * factor * total).astype(jnp.bfloat16)
                res[u, r, :] = now
                dst[slot, rr, :] = norm(now.astype(jnp.float32), gains[...])

            ag_copy(u, 1, k, dst).start()
            ag_copy(u, 0, k, dst).start()

    def ag_rows(k, side):
        return pl.ds(side * SH + k * CHUNK, CHUNK)

    def ag_copy(u, kind, k, buf):
        me, ot, partner = SIDES[u + 1]
        b = buf.at[ot if kind == 2 else me, ag_rows(k, c)]
        return rcopy(b, b, ag_send.at[u, kind, k], ag_recv.at[u, kind, k], partner if kind == 1 else dc)

    def ag_wait(u, kind, k, buf):
        me, ot, _ = SIDES[u + 1]
        b = buf.at[me if kind == 0 else ot, ag_rows(k, c if kind == 1 else oc)]
        rcopy(b, b, ag_send.at[u, kind, k], ag_recv.at[u, kind, k], dc).wait_recv()

    def ag_pass(u, buf, first, last):
        for k in range(first, last):
            ag_wait(u, 1, k, buf)
            ag_copy(u, 2, k, buf).start()

    def ag_own(u, buf):
        for k in range(K):
            ag_wait(u, 0, k, buf)

    def ag_other(u, buf):
        for k in range(K):
            ag_wait(u, 2, k, buf)

    def fc_copy(s, q):
        cols = pl.ds(q * DC, DC)
        return rcopy(part.at[s, orows, cols], rc.at[2, s, :, cols], fc_send.at[s, q], fc_recv.at[s, q], dc)

    def fy_copy(q):
        cols = pl.ds(q * DC, DC)
        return rcopy(ys.at[2, :, cols], ry.at[2, :, cols], fy_send.at[q], fy_recv.at[q], dz)

    def last_push(q):
        cols = pl.ds(q * DC, DC)
        fc_copy(oa, q).wait_recv()

        @pl.loop(0, SH // ROWS)
        def _(i):
            r = pl.ds(i * ROWS, ROWS)
            p = part[oa, pl.ds(c * SH + i * ROWS, ROWS), cols].astype(jnp.float32)
            ys[2, r, cols] = (p + rc[2, oa, r, cols].astype(jnp.float32)).astype(jnp.bfloat16)

        fy_copy(q).start()

    def out_copies(q):
        cols = pl.ds(q * DC, DC)
        src, dst = res.at[2, :, cols], out.at[crows, cols]
        return pltpu.make_async_copy(src, dst, out_sem.at[q]), rcopy(src, dst, oc_send.at[q], oc_recv.at[q], dc)

    def last_finish(q):
        cols = pl.ds(q * DC, DC)
        fc_copy(a, q).wait_recv()
        fy_copy(q).wait_recv()

        @pl.loop(0, SH // ROWS)
        def _(i):
            r = pl.ds(i * ROWS, ROWS)
            total = part[a, pl.ds(c * SH + i * ROWS, ROWS), cols].astype(jnp.float32) + rc[2, a, r, cols].astype(jnp.float32)
            total = total + ry[2, r, cols].astype(jnp.float32)
            res[2, r, cols] = (res[1, r, cols].astype(jnp.float32) + 0.5 * dsc[0:1, cols] * total).astype(jnp.bfloat16)

        for cp in out_copies(q):
            cp.start()

    def value_glu(s):
        @pl.loop(0, C // TILE)
        def _(j):
            lo = pl.multiple_of(j * TILE, TILE)
            rows = xb[s]
            vw = wb2[:, :, pl.ds(lo, TILE)].reshape(D, TILE)
            gw = wb2[:, :, pl.ds(C + lo, TILE)].reshape(D, TILE)
            vv = jnp.dot(rows, vw, preferred_element_type=jnp.float32) * value_scale[:, pl.ds(pl.multiple_of(y * C + lo, LANES), TILE)]
            gv = jnp.dot(rows, gw, preferred_element_type=jnp.float32) * glu_scale[:, pl.ds(pl.multiple_of(y * C + lo, LANES), TILE)]
            g = (vv * jax.nn.sigmoid(gv)).astype(jnp.bfloat16)
            gp[s, pl.ds(PAD, S), pl.ds(lo, TILE)] = g.astype(jnp.float32)

    def convolve(s):
        @pl.loop(0, C // LANES)
        def _(j):
            cols = pl.ds(pl.multiple_of(j * LANES, LANES), LANES)
            near = pl.ds(pl.multiple_of(y * C + j * LANES, LANES), LANES)
            gp[s, pl.ds(0, PAD), cols] = jnp.zeros((PAD, LANES), jnp.float32)
            total = jnp.zeros((S, LANES), jnp.float32)
            for k in range(KW):
                total = total + conv_k[k:k + 1, near] * gp[s, pl.ds(PAD - (KW - 1) + k, S), cols]
            mixed[s, :, cols] = total

        m = mixed[s]
        low = lax.broadcasted_iota(jnp.int32, (8, C), 0) < 4
        one, nil = jnp.ones((8, C), jnp.float32), jnp.zeros((8, C), jnp.float32)
        hi = lax.Precision.HIGHEST
        sums = lax.dot_general(jnp.where(low, one, nil), m, NT, precision=hi, preferred_element_type=jnp.float32)
        squares = lax.dot_general(jnp.where(low, nil, one), m * m, NT, precision=hi, preferred_element_type=jnp.float32)
        st[0, s] = sums + squares

    def st_copies():
        return [rcopy(st.at[0], st.at[k + 1], st_send.at[k], st_recv.at[k], dev) for k, dev in enumerate((dc, dy, dyc))]

    def activate(s):
        total = st[0, s] + st[1, s] + st[2, s] + st[3, s]
        total = total / D
        mean, square = total[0:1], total[4:5]
        rstd = lax.rsqrt(square - mean * mean + EPSILON)
        row = lax.broadcasted_iota(jnp.int32, (8, S), 0)
        both = jnp.where(row == 0, jnp.broadcast_to(mean, (8, S)), jnp.where(row == 1, jnp.broadcast_to(rstd, (8, S)), 0.0))
        pick = lax.broadcasted_iota(jnp.int32, (8, LANES), 0)
        hi = lax.Precision.HIGHEST
        mcol = lax.dot_general(both, jnp.where(pick == 0, 1.0, 0.0), TN, precision=hi, preferred_element_type=jnp.float32)
        rcol = lax.dot_general(both, jnp.where(pick == 1, 1.0, 0.0), TN, precision=hi, preferred_element_type=jnp.float32)
        for j in range(C // LANES):
            cols = slice(j * LANES, (j + 1) * LANES)
            v = (mixed[s, :, cols] - mcol) * rcol * norm_gain[:, pl.ds(pl.multiple_of(y * C + j * LANES, LANES), LANES)]
            act[s, :, cols] = (v * jax.nn.sigmoid(v)).astype(jnp.bfloat16)

    tok_local.wait()
    norm_tokens(a)
    ff_arrive(0, 1)
    ff_y_own(0, 1)
    ff_own(1)
    ff_arrive(0, 2)
    ff_relay(0, 1)
    for d in range(3, Z):
        ff_arrive(0, d)
    y_start(2, 0)
    y_start(3, 0)
    ff_y_own(1, 0)
    ff_arrive(1, 1)
    ff_relay(0, 2)
    rcopy(there, there, tok_sem.at[0], tok_sem.at[1], dz).wait_recv()
    tok_core.start()
    send_rows(2, f, False)
    send_rows(3, f, False)
    send_rows(2, fp, True)
    send_rows(3, fp, True)
    ff_arrive(1, 2)
    for d in range(3, Z):
        ff_arrive(1, d)
    ff_y_own(1, 1)
    for d in range(3, Z):
        ff_relay(0, d)
    b = tokv.at[oa, orows]
    rcopy(b, b, tok_sem.at[2], tok_sem.at[3], dc).wait_recv()
    norm_tokens(oa)
    forward(2, 1)
    forward(2, 2)
    ff_relay(1, 1)
    ff_relay(1, 2)
    for d in range(3, Z):
        forward(2, d)
    for d in range(3, Z):
        ff_relay(1, d)
    forward(3, 1)
    forward(3, 2)
    ff_done(0)
    gate_up(xa, oa)
    for d in range(3, Z):
        forward(3, d)
    gate_up(xa, a)
    ff_done(1)
    y_start(2, 1)
    y_start(3, 1)
    project(hid, wb1, H, oa)
    rs_core(0, oa).start()
    project(hid, wb1, H, a)
    rs_core(0, a).start()
    rs_push(0)
    for j in range(1, F):
        b = scl.at[lax.rem(f + j, F)]
        rcopy(b, b, s_send.at[j], s_recv.at[lax.rem(f + j, F)], dy).wait_recv()
    scl[f] = sc[...]
    for j in range(F):
        dsc[:, j * R:(j + 1) * R] = scl[j]
    rs_finish(0, None, 0.5, 0, conv_gain, xb)
    ag_pass(0, xb, 0, K)
    ag_own(0, xb)
    group_done(2)
    value_glu(y)
    convolve(y)
    ag_other(0, xb)
    value_glu(oy)
    convolve(oy)
    for cp in st_copies():
        cp.start()
    for s in range(2):
        rs_core(0, s).wait_send()
    for cp in st_copies():
        cp.wait()
    group_done(3)
    activate(oy)
    project(act, wb3, C, oy)
    rs_core(1, oy).start()
    activate(y)
    project(act, wb3, C, y)
    rs_core(1, y).start()
    rs_push(1)
    for g in (0, 1):
        ff_drain(g)
    for g in (2, 3):
        drain(g)
    rs_finish(1, 0, 1.0, 1, second_gain, xc)
    ag_own(1, xc)
    gate_up(xc, a)
    for s in range(2):
        rs_core(1, s).wait_send()
    ag_pass(1, xc, 0, K)
    ag_other(1, xc)
    gate_up(xc, oa)
    step = F // COLS
    for q in range(COLS):
        project(hid, wb1, H, oa, q * step, (q + 1) * step)
        fc_copy(oa, q).start()
        if q:
            last_push(q - 1)
    for q in range(COLS):
        project(hid, wb1, H, a, q * step, (q + 1) * step)
        fc_copy(a, q).start()
        if q == 0:
            last_push(COLS - 1)
    tok_z.wait_send()
    tok_core.wait_send()
    for j in range(1, F):
        rcopy(sc, scl.at[f], s_send.at[j], s_recv.at[f], dy).wait_send()
    for u, buf in enumerate((xb, xc)):
        for k in range(K):
            rs_pair(u, k).wait_send()
            for kind in range(3):
                ag_copy(u, kind, k, buf).wait_send()
    for q in range(COLS):
        last_finish(q)
    for q in range(COLS):
        for s in range(2):
            fc_copy(s, q).wait_send()
        fy_copy(q).wait_send()
        near, far = out_copies(q)
        near.wait()
        far.wait_send()
        b = out.at[orows, pl.ds(q * DC, DC)]
        rcopy(b, b, oc_send.at[q], oc_recv.at[q], dc).wait_recv()


def local_fused(tokens, gate_weight, up_weight, down_weight, value_weight, glu_weight, out_weight, gate_scale, up_scale,
                down_scale, value_scale, glu_scale, out_scale, conv_kernel, norm_gain, first_gain, conv_gain, second_gain):
    F = lax.axis_size("fs")
    S, D = tokens.shape
    R, H = gate_weight.shape[0], gate_weight.shape[1] // 2
    C = value_weight.shape[1] // 2
    KW = conv_kernel.shape[0]
    RX = R // 2
    SH = S // 2
    vectors = (down_scale, out_scale, first_gain, conv_gain, second_gain, gate_scale, up_scale, value_scale, glu_scale, norm_gain)
    rows = [v.reshape(-1, LANES) if v is gate_scale or v is up_scale else v.reshape(1, -1) for v in vectors]
    widths = (2 * H, H, 2 * C, C)
    G, K, NS = len(widths), SH // CHUNK, max(SUBS)
    bf, f32 = jnp.bfloat16, jnp.float32
    dma = pltpu.SemaphoreType.DMA
    anyspace = pl.BlockSpec(memory_space=pl.ANY)
    vmem = pl.BlockSpec(memory_space=pltpu.VMEM)
    pad = -(-(KW - 1) // 8) * 8
    return pl.pallas_call(
        functools.partial(fused_kernel, (S, D, H, C, KW, F, RX)),
        out_shape=jax.ShapeDtypeStruct((S, D), bf),
        in_specs=[anyspace] * 7 + [vmem] * 11,
        out_specs=anyspace,
        scratch_shapes=[pltpu.VMEM((2 * F, RX, w), bf) for w in widths]
        + [pltpu.VMEM((1 if g < 2 else 2, RX, w), bf) for g, w in enumerate(widths)]
        + [pltpu.VMEM((2, R, 2 * H), f32)]
        + [pltpu.VMEM((2, S, D), bf)] * 4
        + [pltpu.VMEM((2, S, H), bf), pltpu.VMEM((2, S, D), bf)]
        + [pltpu.VMEM((3, 2, SH, D), bf), pltpu.VMEM((3, SH, D), bf), pltpu.VMEM((3, SH, D), bf), pltpu.VMEM((3, SH, D), bf)]
        + [pltpu.VMEM((2, S + pad, C), f32), pltpu.VMEM((2, S, C), f32), pltpu.VMEM((2, S, C), bf)]
        + [pltpu.VMEM((4, 2, 8, S), f32), pltpu.VMEM((8, R), f32), pltpu.VMEM((F, 8, R), f32), pltpu.VMEM((8, D), f32)]
        + [dma((2, 2)), dma((G, F // 2, 2, NS)), dma((G, F // 2, 2, NS))] + [dma((G, F, NS))] * 2 + [dma((2, 2, NS))] + [dma((G, F, NS))] * 3
        + [dma((4,)), dma((F,)), dma((F,))]
        + [dma((3, 2)), dma((3, 2)), dma((2, K)), dma((2, K)), dma((2, 3, K)), dma((2, 3, K))]
        + [dma((2, COLS)), dma((2, COLS)), dma((COLS,)), dma((COLS,))]
        + [dma((3,)), dma((3,)), dma((COLS,)), dma((COLS,)), dma((COLS,))],
        compiler_params=pltpu.CompilerParams(
            collective_id=0, has_side_effects=True, vmem_limit_bytes=64 * 1024 * 1024 - 65536
        ),
    )(tokens, gate_weight, up_weight, down_weight, value_weight, glu_weight, out_weight, *rows, conv_kernel)


def rms_rows(rows, gains):
    values = rows.astype(jnp.float32)
    scaled = values * lax.rsqrt(jnp.mean(values * values, axis=-1, keepdims=True) + EPSILON)
    return (scaled * gains).astype(jnp.bfloat16)


def gated_hidden(normed, gate_full, up_full, gate_scale, up_scale):
    gate_part = jnp.dot(normed, gate_full, preferred_element_type=jnp.float32) * gate_scale
    upward = jnp.dot(normed, up_full, preferred_element_type=jnp.float32) * up_scale
    return (jax.nn.silu(gate_part) * upward).astype(jnp.bfloat16)


def causal_depthwise(inputs, kernel):
    taps = kernel.shape[0]
    length = inputs.shape[0]
    padded = jnp.concatenate(
        [jnp.zeros((taps - 1, inputs.shape[1]), jnp.float32), inputs.astype(jnp.float32)], axis=0
    )
    total = jnp.zeros((length, inputs.shape[1]), jnp.float32)
    for offset in range(taps):
        total = total + kernel[offset] * padded[offset : offset + length]
    return total


def swap(values, axis):
    return lax.ppermute(values, axis, [(0, 1), (1, 0)])


def gather_rows(rows, axis):
    if lax.axis_size(axis) != 2:
        return lax.all_gather(rows, axis, axis=0, tiled=True)
    other = swap(rows, axis)
    first = lax.axis_index(axis) == 0
    return jnp.concatenate([jnp.where(first, rows, other), jnp.where(first, other, rows)], axis=0)


def scatter_rows(partial, axis):
    members = lax.axis_size(axis)
    if members != 2:
        return lax.psum_scatter(partial, axis, scatter_dimension=0, tiled=True).astype(jnp.float32)
    own_rows = partial.shape[0] // members
    place = lax.axis_index(axis)
    mine = lax.dynamic_slice_in_dim(partial, place * own_rows, own_rows, 0)
    theirs = lax.dynamic_slice_in_dim(partial, (1 - place) * own_rows, own_rows, 0)
    return mine.astype(jnp.float32) + swap(theirs, axis).astype(jnp.float32)


def pull(rows, step):
    n = lax.axis_size("rep")
    return lax.ppermute(rows, "rep", [(s, (s - step) % n) for s in range(n)])


def push(rows, step):
    n = lax.axis_size("rep")
    return lax.ppermute(rows, "rep", [(s, (s + step) % n) for s in range(n)])


def streams_of(own):
    n = lax.axis_size("rep")
    parts = [own] + [pull(own, step) for step in range(1, n)]
    return [gather_rows(part, "tp") for part in parts]


def owned_sum(actives, weight_rows):
    n = lax.axis_size("rep")
    total = None
    for step in list(range(1, n)) + [0]:
        partial = lax.dot_general(
            actives[step], weight_rows, (((1,), (1,)), ((), ())), preferred_element_type=jnp.float32
        ).astype(jnp.bfloat16)
        part = scatter_rows(partial, "tp")
        if step:
            part = push(part.astype(jnp.bfloat16), step).astype(jnp.float32)
        total = part if total is None else total + part
    return total


def local_plain(
    tokens,
    gate_weight,
    up_weight,
    down_weight,
    value_weight,
    glu_weight,
    out_weight,
    gate_scale,
    up_scale,
    down_scale,
    value_scale,
    glu_scale,
    out_scale,
    conv_kernel,
    norm_gain,
    first_gain,
    conv_gain,
    second_gain,
):
    reps = lax.axis_size("rep")
    rep = lax.axis_index("rep")

    def part(array, dim):
        width = array.shape[dim] // reps
        return lax.dynamic_slice_in_dim(array, rep * width, width, dim)

    scales = lax.all_gather(jnp.stack([down_scale, out_scale]), "fs", axis=1, tiled=True)
    down_rows, out_rows = scales[0], scales[1]

    def full(weight):
        return lax.all_gather(part(weight, 1).astype(jnp.bfloat16), "fs", axis=0, tiled=True)

    gate_full, up_full, down_full, value_full, glu_full, out_full = (
        full(gate_weight),
        full(up_weight),
        full(down_weight),
        full(value_weight),
        full(glu_weight),
        full(out_weight),
    )
    gate_scale, up_scale, value_scale, glu_scale, norm_gain = (
        part(gate_scale, 0),
        part(up_scale, 0),
        part(value_scale, 0),
        part(glu_scale, 0),
        part(norm_gain, 0),
    )
    conv_kernel = part(conv_kernel, 1)
    members = lax.axis_size("tp")
    own_rows = tokens.shape[0] // members
    own_tokens = lax.dynamic_slice_in_dim(tokens, lax.axis_index("tp") * own_rows, own_rows, 0)

    normed = rms_rows(tokens, first_gain)
    own_normed = rms_rows(own_tokens, first_gain)
    rows = [normed] + [gather_rows(pull(own_normed, step), "tp") for step in range(1, reps)]
    hidden = [gated_hidden(r, gate_full, up_full, gate_scale, up_scale) for r in rows]
    after_first = (
        own_tokens.astype(jnp.float32) + 0.5 * down_rows * owned_sum(hidden, down_full)
    ).astype(jnp.bfloat16)
    mixes, sums = [], []
    for rows in streams_of(rms_rows(after_first, conv_gain)):
        value_part = jnp.dot(rows, value_full, preferred_element_type=jnp.float32) * value_scale
        gate_part = jnp.dot(rows, glu_full, preferred_element_type=jnp.float32) * glu_scale
        glu_in = (value_part * jax.nn.sigmoid(gate_part)).astype(jnp.bfloat16)
        mixed = causal_depthwise(glu_in, conv_kernel)
        mixes.append(mixed)
        sums.append(jnp.stack([jnp.sum(mixed, axis=1), jnp.sum(mixed * mixed, axis=1)]))
    totals = lax.psum(jnp.roll(jnp.stack(sums), rep, axis=0), ("rep", "tp"))
    totals = jnp.roll(totals, -rep, axis=0) / (norm_gain.shape[0] * reps * lax.axis_size("tp"))
    actives = []
    for step, mixed in enumerate(mixes):
        mean_rows = totals[step, 0][:, None]
        square_rows = totals[step, 1][:, None]
        normalized = (
            (mixed - mean_rows) * lax.rsqrt(square_rows - mean_rows * mean_rows + EPSILON) * norm_gain
        )
        actives.append(jax.nn.silu(normalized).astype(jnp.bfloat16))
    after_conv = (after_first.astype(jnp.float32) + out_rows * owned_sum(actives, out_full)).astype(
        jnp.bfloat16
    )
    hidden = [
        gated_hidden(r, gate_full, up_full, gate_scale, up_scale)
        for r in streams_of(rms_rows(after_conv, second_gain))
    ]
    after_second = (
        after_conv.astype(jnp.float32) + 0.5 * down_rows * owned_sum(hidden, down_full)
    ).astype(jnp.bfloat16)
    return gather_rows(after_second, "tp")


def fits(mesh):
    return mesh.shape["rep"] == 2 and mesh.shape["tp"] == 2 and mesh.shape["fs"] % 4 == 0


def solution(mesh):
    columns, rows = P("fs", "tp"), P(("rep", "fs"), None)
    placed = (rows,) + (columns,) * 6 + (P("tp"), P("tp"), P("fs"), P("tp"), P("tp"), P("fs"), P(None, "tp"), P("tp"), P(), P(), P())
    local = local_fused if fits(mesh) else local_plain
    return jax.shard_map(local, mesh=mesh, in_specs=placed, out_specs=rows, check_vma=False)
```
